512 devices in a mesh: sp: 64 (over z, y), tp: 8 (over x, core).
Axes of the slice: x: 4, y: 4, z: 16, core: 2. Of those that a mesh axis runs over, the one named last changes fastest.
Arguments:
- receptance: bfloat16 [12288, 1024], P('sp', 'tp'), may hold values from -6 to 6
- head_keys: bfloat16 [12288, 1024], P('sp', 'tp'), may hold values from -6 to 6
- head_values: bfloat16 [12288, 1024], P('sp', 'tp'), may hold values from -6 to 6
- decay_preact: float32 [12288, 1024], P('sp', 'tp'), may hold values from -13.5 to -0.5
- learning_rate_preact: float32 [12288, 1024], P('sp', 'tp'), may hold values from -10.5 to 2.5
- output_gate_preact: bfloat16 [12288, 1024], P('sp', 'tp'), may hold values from -8 to 8
- self_token_weight: float32 [16, 64], P('tp'), may hold values from -0.6 to 0.6
- head_norm_gain: float32 [1024], P('tp'), may hold values from 0.1 to 1.9
- output_weight: bfloat16 [1024, 2048], P('tp'), may hold values from -0.1875 to 0.1875
- residual: bfloat16 [12288, 2048], P('sp'), may hold values from -6 to 6
- premixer_norm_gain: float32 [2048], replicated, may hold values from 0.1 to 1.9
- mixer_gate_weight: bfloat16 [2048, 5120], P('sp', 'tp'), may hold values from -0.125 to 0.125
- mixer_up_weight: bfloat16 [2048, 5120], P('sp', 'tp'), may hold values from -0.125 to 0.125
- mixer_down_weight: bfloat16 [5120, 2048], P('tp', 'sp'), may hold values from -0.078125 to 0.078125
Outputs:
- layer_out: bfloat16 [12288, 2048], P(('sp', 'tp'))
The draws below stay inside these ranges and needn't reach their ends.
All inputs are finite; a program needn't handle non-finite values.
Results may differ from the reference program's by a relative error of at most 0.015.
Values may be sent and summed in bfloat16 or wider, within the bound.
A program may use at most 64 MiB of HBM per device.

```python
import jax
import jax.numpy as jnp
from jax import lax

D = 2048
WIDTH = 1024
HEAD_SIZE = 64
RECURRENT_HEADS = 16
FF = 5120
TOK_DEV = 192
TOKENS = 12288
N_TP = 8


def head_speed(key):
    chosen = jax.random.permutation(jax.random.fold_in(key, 4711), WIDTH // HEAD_SIZE)
    fast_count = WIDTH // HEAD_SIZE // 2
    return chosen < fast_count


def draw_decay_preact(key, part):
    fast_heads = head_speed(key)
    head_total = WIDTH // HEAD_SIZE
    keys_all = jax.random.split(jax.random.fold_in(key, 17), 5)
    fast_base = jax.random.uniform(keys_all[0], (head_total,), jnp.float32, -3.5, -2.5)
    slow_base = jax.random.uniform(keys_all[1], (head_total,), jnp.float32, -11.5, -10.5)
    head_base = jnp.where(fast_heads, fast_base, slow_base)
    shards = TOKENS // TOK_DEV
    block_shift = jax.random.uniform(keys_all[2], (shards, head_total), jnp.float32, -1.0, 1.0)
    block_shift = jnp.repeat(block_shift, TOK_DEV, axis=0)
    jitter = jax.random.uniform(keys_all[3], (TOKENS, head_total, HEAD_SIZE), jnp.float32, -1.0, 1.0)
    return (head_base[None, :, None] + block_shift[:, :, None] + jitter).reshape(TOKENS, WIDTH)


def draw_learning_rate_preact(key, part):
    fast_heads = head_speed(key)
    head_total = WIDTH // HEAD_SIZE
    keys_all = jax.random.split(jax.random.fold_in(key, 29), 2)
    fast_part = jax.random.uniform(keys_all[0], (TOKENS, head_total, HEAD_SIZE), jnp.float32, -2.5, 2.5)
    slow_part = jax.random.uniform(keys_all[1], (TOKENS, head_total, HEAD_SIZE), jnp.float32, -10.5, -7.5)
    return jnp.where(fast_heads[None, :, None], fast_part, slow_part).reshape(TOKENS, WIDTH)


def block_scale(own_key, dims, cuts, smallest, high):
    factor_of, own = 1.0, jax.random.fold_in(own_key, 6)
    for axis_at, shards_of in cuts:
        draws = jnp.exp(jax.random.uniform(jax.random.fold_in(own, axis_at), (shards_of,), jnp.float32, smallest / len(cuts), high / len(cuts)))
        factor_of = factor_of * jnp.repeat(draws, dims[axis_at] // shards_of).reshape([-1 if axis == axis_at else 1 for axis in range(len(dims))])
    return factor_of


def centred(key, shape, scale, most, cuts=(), held_as=jnp.bfloat16):
    drawn = jax.random.normal(key, shape, jnp.float32) * scale
    if len(cuts) > 0:
        drawn = block_scale(key, shape, cuts, -0.22, 0.18) * drawn
    return jnp.clip(drawn, min=-most, max=most).astype(held_as)


def setup_inputs(seed: int = 0) -> dict:
    keys = jax.random.split(jax.random.key(seed), 15)
    return {
        "receptance": centred(keys[0], (TOKENS, WIDTH), 1.0, 6.0, ((0, 64), (1, 8))),
        "head_keys": centred(keys[1], (TOKENS, WIDTH), 1.0, 6.0, ((0, 64), (1, 8))),
        "head_values": centred(keys[2], (TOKENS, WIDTH), 1.0, 6.0, ((0, 64), (1, 8))),
        "decay_preact": draw_decay_preact(jax.random.fold_in(keys[14], 71), 0),
        "learning_rate_preact": draw_learning_rate_preact(jax.random.fold_in(keys[14], 71), 0),
        "output_gate_preact": centred(keys[5], (TOKENS, WIDTH), 1.5, 8.0, ((0, 64), (1, 8))),
        "self_token_weight": centred(keys[6], (RECURRENT_HEADS, HEAD_SIZE), 0.1, 0.6, ((0, 8),), jnp.float32),
        "head_norm_gain": jnp.clip(1.0 + 0.18 * jax.random.normal(keys[7], (WIDTH,), jnp.float32), 0.1, 1.9),
        "output_weight": centred(keys[8], (WIDTH, D), WIDTH ** -0.5, 0.1875, ((0, 8),)),
        "residual": centred(keys[9], (TOKENS, D), 1.0, 6.0, ((0, 64),)),
        "premixer_norm_gain": jnp.clip(1.0 + 0.18 * jax.random.normal(keys[10], (D,), jnp.float32), 0.1, 1.9),
        "mixer_gate_weight": centred(keys[11], (D, FF), D ** -0.5, 0.125, ((0, 64), (1, 8))),
        "mixer_up_weight": centred(keys[12], (D, FF), D ** -0.5, 0.125, ((0, 64), (1, 8))),
        "mixer_down_weight": centred(keys[13], (FF, D), FF ** -0.5, 0.078125, ((0, 8), (1, 64))),
    }


GROUP_EPS = 0.00064
NORM_EPS = 1e-06
EXACT = lax.Precision.HIGHEST

def final_output(layer_result, receptance_rows, keys_single, values_single, self_token_weight, head_norm_gain, output_gate_preact):
    centre = lax.optimization_barrier(jnp.mean(layer_result, axis=-1, keepdims=True))
    spread = lax.optimization_barrier(jnp.mean(jnp.square(layer_result - centre), axis=-1, keepdims=True))
    scaled_rows = (layer_result - centre) * lax.rsqrt(spread + GROUP_EPS)
    self_token_term = lax.optimization_barrier(jnp.sum(receptance_rows * keys_single * self_token_weight[None], axis=-1, keepdims=True)) * values_single
    sequence_length = layer_result.shape[0]
    heads_merged = scaled_rows.reshape(sequence_length, -1) * head_norm_gain[None] + self_token_term.reshape(sequence_length, -1)
    return (heads_merged * jax.nn.sigmoid(output_gate_preact.astype(jnp.float32))).astype(jnp.bfloat16)

def reference(receptance, head_keys, head_values, decay_preact, learning_rate_preact, output_gate_preact, self_token_weight, head_norm_gain, output_weight, residual, premixer_norm_gain, mixer_gate_weight, mixer_up_weight, mixer_down_weight):
    sequence_length = receptance.shape[0]
    head_count = WIDTH // HEAD_SIZE
    layout = (sequence_length, head_count, HEAD_SIZE)
    receptance_rows = receptance.astype(jnp.float32).reshape(layout)
    keys_single = head_keys.astype(jnp.float32).reshape(layout)
    values_single = head_values.astype(jnp.float32).reshape(layout)
    decay_rate = jnp.exp(-jnp.exp(-jax.nn.softplus(-decay_preact) - 0.5)).reshape(layout)
    learn_rate = jax.nn.sigmoid(learning_rate_preact).reshape(layout)
    unit_key = keys_single / jnp.maximum(jnp.linalg.norm(keys_single, axis=-1, keepdims=True), 1.0)
    remove_dir = -unit_key
    insert_dir = unit_key * learn_rate

    def advance(memory, inputs):
        decay_t, key_t, value_t, remove_t, insert_t, recept_t = inputs
        erased = jnp.einsum('hij,hj->hi', memory, remove_t, precision=EXACT)
        memory = memory * decay_t[:, None, :] + erased[:, :, None] * insert_t[:, None, :] + value_t[:, :, None] * key_t[:, None, :]
        return (memory, jnp.einsum('hij,hj->hi', memory, recept_t, precision=EXACT))
    start_state = jnp.zeros((head_count, HEAD_SIZE, HEAD_SIZE), jnp.float32)
    _, recurrence_output = lax.scan(advance, start_state, (decay_rate, keys_single, values_single, remove_dir, insert_dir, receptance_rows))
    mixer_output = final_output(recurrence_output, receptance_rows, keys_single, values_single, self_token_weight, head_norm_gain, output_gate_preact)
    group = WIDTH // N_TP

    def add_group(total, which):
        begin = (which * group).astype(jnp.int32)
        columns = lax.dynamic_slice_in_dim(mixer_output, begin, group, 1)
        rows_part = lax.dynamic_slice_in_dim(output_weight, begin, group, 0)
        product = jnp.dot(columns.astype(jnp.float32), rows_part.astype(jnp.float32), preferred_element_type=jnp.float32)
        return (total + lax.optimization_barrier(product.astype(jnp.bfloat16)).astype(jnp.float32), None)
    mix_sum, _ = lax.scan(add_group, jnp.zeros((sequence_length, D), jnp.float32), jnp.arange(N_TP, dtype=jnp.int32))
    mix = lax.optimization_barrier(mix_sum.astype(jnp.bfloat16)).astype(jnp.float32)
    after_mix = (residual.astype(jnp.float32) + mix).astype(jnp.bfloat16)
    widened = after_mix.astype(jnp.float32)
    normed = (widened * lax.rsqrt(lax.optimization_barrier(jnp.mean(widened * widened, axis=-1, keepdims=True)) + NORM_EPS) * premixer_norm_gain[None]).astype(jnp.bfloat16)
    hidden_group = FF // N_TP

    def add_hidden(total, which):
        begin = (which * hidden_group).astype(jnp.int32)
        gate_sum = jnp.dot(normed.astype(jnp.float32), lax.dynamic_slice_in_dim(mixer_gate_weight, begin, hidden_group, 1).astype(jnp.float32), preferred_element_type=jnp.float32)
        up_sum = jnp.dot(normed.astype(jnp.float32), lax.dynamic_slice_in_dim(mixer_up_weight, begin, hidden_group, 1).astype(jnp.float32), preferred_element_type=jnp.float32)
        hidden = (jax.nn.silu(gate_sum) * up_sum).astype(jnp.bfloat16)
        product = jnp.dot(hidden.astype(jnp.float32), lax.dynamic_slice_in_dim(mixer_down_weight, begin, hidden_group, 0).astype(jnp.float32), preferred_element_type=jnp.float32)
        return (total + lax.optimization_barrier(product.astype(jnp.bfloat16)).astype(jnp.float32), None)
    down_sum, _ = lax.scan(add_hidden, jnp.zeros((sequence_length, D), jnp.float32), jnp.arange(N_TP, dtype=jnp.int32))
    return (after_mix.astype(jnp.float32) + down_sum).astype(jnp.bfloat16)
```

```python
import functools
import math

import jax
import jax.numpy as jnp
from jax import lax
from jax.experimental import pallas as pl
from jax.experimental.pallas import tpu as pltpu
from jax.sharding import Mesh
from jax.sharding import PartitionSpec as P

F32, BF16 = jnp.float32, jnp.bfloat16
EXACT = lax.Precision.HIGHEST
MESH = pl.DeviceIdType.MESH
GROUP_EPS = 0.00064
NORM_EPS = 1e-06

NZ, NY, NX, NC = 16, 4, 4, 2
N = 192
ROWS = 24
D = 2048
FF = 640
W = 32


def dot(a, b, ca=1, cb=0):
    return lax.dot_general(
        a.astype(BF16), b.astype(BF16), (((ca,), (cb,)), ((), ())), preferred_element_type=F32
    )


def dotx(a, b, ca=1, cb=0):
    return lax.dot_general(
        a, b, (((ca,), (cb,)), ((), ())), precision=EXACT, preferred_element_type=F32
    )


def iota(shape, d):
    return lax.broadcasted_iota(jnp.int32, shape, d)


def head_ones():
    return jnp.where(iota((128, 128), 0) // 64 == iota((128, 128), 1) // 64, 1.0, 0.0).astype(F32)


def invert(low):
    n = low.shape[0]
    row, col = iota((n, n), 0), iota((n, n), 1)
    eye = jnp.where(row == col, 1.0, 0.0).astype(F32)
    d = jnp.where(row // 8 == col // 8, low, 0.0)
    d2 = dotx(d, d)
    d4 = dotx(d2, d2)
    x = eye + d
    x = x + dotx(d2, x)
    x = x + dotx(d4, x)
    m = 8
    while m < 64:
        off = jnp.where((row // (2 * m) == col // (2 * m)) & (row // m != col // m), low, 0.0)
        x = x + dot(x, dot(off, x))
        m *= 2
    off = jnp.where(row // 64 != col // 64, low, 0.0)
    y = dot(x, off)
    z = dot(y, x)
    return x + z + dot(y, z)


def local_scan(r, k, v, dec, lr, service):
    r, k, v = r.astype(F32), k.astype(F32), v.astype(F32)
    lw = (-math.exp(-0.5)) / (1.0 + jnp.exp(-dec))
    row, col = iota((N, N), 0), iota((N, N), 1)
    c = dotx(jnp.where(row >= col, 1.0, 0.0).astype(F32), lw)
    norm = jnp.sqrt(dotx(k * k, head_ones()))
    unit = k / jnp.maximum(norm, 1.0)
    ins = unit / (1.0 + jnp.exp(-lr))
    up, dn = jnp.exp(c), jnp.exp(-c)
    last = c[N - 1 : N]
    rest = jnp.exp(last - c)
    at = -unit * jnp.exp(c - lw)
    rt = r * up
    left = jnp.concatenate([at, rt], 0)
    right = jnp.concatenate([ins * dn, k * dn], 0).astype(BF16)
    lane2 = iota((N, 256), 1) % 128
    us, outs = [], []
    for h in range(2):
        head_lanes = iota((2 * N, 128), 1) // 64 == h
        g = dot(jnp.where(head_lanes, left, 0.0), right, 1, 1)
        low = jnp.where(row > col, g[:N, :N], 0.0)
        mak = jnp.where(row > col, g[:N, N:], 0.0)
        mrb = jnp.where(row >= col, g[N:, :N], 0.0)
        mrk = jnp.where(row >= col, g[N:, N:], 0.0)
        x = invert(low)
        u = dot(x, jnp.concatenate([at, dot(mak, v)], 1))
        o = dot(mrb, u)
        ov = dot(mrk, v)
        us.append(u)
        outs.append(jnp.concatenate([o[:, :128] + rt, o[:, 128:] + ov], 1))
        service()
    u = jnp.where(lane2 < 64, us[0], us[1])
    o = jnp.where(lane2 < 64, outs[0], outs[1])
    f = dot((ins * rest).T, u)
    fl = f[:, 128:] + dot((k * rest).T, v)
    ones = head_ones()
    r1, c1 = iota((128, 128), 0), iota((128, 128), 1)
    e = f[:, :128] * ones + jnp.where(r1 == c1, jnp.exp(last) - 1.0, 0.0)
    l = fl * ones
    return e[:64] + e[64:], l[:64] + l[64:], o


def unpack(p):
    first = iota(p.shape, 1) % 128 < 64
    return jnp.concatenate([jnp.where(first, p, 0.0), jnp.where(first, 0.0, p)], 0)


def pack(p):
    first = iota((64, p.shape[1]), 1) % 128 < 64
    return jnp.where(first, p[:64], p[64:])


def kernel(
    r_ref, k_ref, v_ref, dec_ref, lr_ref, og_ref, stw_ref, hng_ref, wo_ref, res_ref, png_ref,
    wg_ref, wu_ref, wd_ref,
    out_ref,
    gu, dn, state, entry_buf, part, pair_in, mine, mix_in, rows_buf, nrm, local_out, resid,
    loc_sem, zs, zr, ys, yr, as_, ar, azs, azr, ss, sr, ps, pr, xs, xr, gs, gr, fs, fr,
):
    z, y, x, core = (lax.axis_index(a) for a in ("z", "y", "x", "c"))
    here = z * NY + y

    def at(dz=0, dy=0, dx=0, dc=0):
        return (
            lax.rem(z + dz + NZ, NZ), lax.rem(y + dy + NY, NY),
            lax.rem(x + dx + NX, NX), lax.rem(core + dc, NC),
        )

    sends = []

    def push(src, dst, send, recv, to):
        cp = pltpu.make_async_remote_copy(
            src_ref=src, dst_ref=dst, send_sem=send, recv_sem=recv, device_id=to,
            device_id_type=MESH,
        )
        cp.start()
        sends.append(cp)
        return cp

    def landed(dst, send, recv):
        pltpu.make_async_remote_copy(
            src_ref=dst, dst_ref=dst, send_sem=send, recv_sem=recv, device_id=at(dz=1),
            device_id_type=MESH,
        ).wait_recv()

    own = [
        pltpu.make_async_copy(wg_ref, gu.at[here, pl.ds(0, W)], loc_sem.at[0]),
        pltpu.make_async_copy(wu_ref, gu.at[here, pl.ds(W, W)], loc_sem.at[1]),
        pltpu.make_async_copy(wd_ref, dn.at[here], loc_sem.at[2]),
    ]
    row0 = pl.multiple_of((x * NC + core) * ROWS, 8)
    fetch = pltpu.make_async_copy(res_ref.at[pl.ds(row0, ROWS)], resid, loc_sem.at[3])
    for cp in own:
        cp.start()
    fetch.start()

    zb, za = z % 4, z // 4
    peers = [at(dz=1), at(dz=-1), at(dy=1), at(dy=2), at(dy=3)]
    peers += [at(dx=d) for d in (1, 2, 3)] + [at(dc=1)]
    z_near = [(za * 4 + lax.rem(zb + d, 4), y, x, core) for d in (1, 2, 3)]
    z_far = [at(dz=4 * d) for d in (1, 2, 3)]
    peers += z_near + z_far
    barrier = pltpu.get_barrier_semaphore()
    for p in peers:
        pl.semaphore_signal(barrier, inc=1, device_id=p, device_id_type=MESH)
    for cp in own:
        cp.wait()
    pl.semaphore_wait(barrier, len(peers))

    def slot(dz, dy=0):
        return lax.rem(z + dz + NZ, NZ) * NY + lax.rem(y + dy + NY, NY)

    def column(dz):
        return pl.multiple_of(lax.rem(z + dz + NZ, NZ) * NY, NY)

    def offsets(s):
        return [0] if s == 0 else ([-s, s] if s < 8 else [8])

    def index(o):
        return 0 if o == 0 else (15 if o == 8 else 2 * abs(o) - (1 if o < 0 else 0))

    def y_out(o):
        i = index(o)
        src = gu.at[slot(o)]
        push(src, src, ys.at[i, 0], yr.at[i, 0], at(dy=1))
        push(src, src, ys.at[i, 1], yr.at[i, 1], at(dy=-1))

    def y_on(o):
        i = index(o)
        a, b = gu.at[slot(o, -1)], gu.at[slot(o, 1)]
        landed(a, ys.at[i, 0], yr.at[i, 0])
        a = gu.at[slot(o, -1), pl.ds(0, W)]
        push(a, a, ys.at[i, 2], yr.at[i, 2], at(dy=1))
        landed(b, ys.at[i, 1], yr.at[i, 1])
        b = gu.at[slot(o, 1), pl.ds(W, W)]
        push(b, b, ys.at[i, 3], yr.at[i, 3], at(dy=-1))

    def y_end(o):
        i = index(o)
        landed(gu.at[slot(o, 2), pl.ds(0, W)], ys.at[i, 2], yr.at[i, 2])
        landed(gu.at[slot(o, 2), pl.ds(W, W)], ys.at[i, 3], yr.at[i, 3])

    def z_block(dz, d, s):
        b = gu.at[slot(dz)]
        return b if s < 8 else gu.at[slot(dz), pl.ds(W * d, W)]

    def z_out(s):
        for d in range(2):
            o = -s if d == 0 else s
            b = z_block(o, d, s + 1)
            push(b, b, zs.at[d, s], zr.at[d, s], at(dz=1 if d == 0 else -1))

    def z_in(s):
        for d in range(2):
            landed(z_block(-s if d == 0 else s, d, s), zs.at[d, s - 1], zr.at[d, s - 1])

    def a_block(dz, d, s):
        return dn.at[pl.ds(column(dz), NY)] if s < 8 else dn.at[pl.ds(column(dz) + 2 * d, 2)]

    def a_out(s):
        for d in range(2):
            b = a_block(-s if d == 0 else s, d, s + 1)
            push(b, b, azs.at[d, s], azr.at[d, s], at(dz=1 if d == 0 else -1))

    def a_in(s):
        for d in range(2):
            b = a_block(-s if d == 0 else s, d, s)
            landed(b, azs.at[d, s - 1], azr.at[d, s - 1])

    turn = [0]

    def service():
        s = turn[0]
        turn[0] += 1
        if s == 0:
            z_out(0)
            for d in (1, 2, 3):
                push(dn.at[here], dn.at[here], as_.at[d - 1], ar.at[d - 1], at(dy=d))
            y_out(0)
        elif s <= 8:
            z_in(s)
            if s < 8:
                z_out(s)
            if s == 1:
                for d in (1, 2, 3):
                    landed(dn.at[slot(0, -d)], as_.at[d - 1], ar.at[d - 1])
            else:
                a_in(s - 1)
            a_out(s - 1)
            for o in offsets(s):
                y_out(o)
            for o in offsets(s - 1):
                y_on(o)
        elif s == 9:
            a_in(8)
            for o in offsets(8):
                y_on(o)
            for t in range(9):
                for o in offsets(t):
                    y_end(o)

    service()

    e, l, o = local_scan(r_ref[...], k_ref[...], v_ref[...], dec_ref[...], lr_ref[...], service)
    local_out[...] = o

    def level(n, x_own, mates, place):
        state[n, place, :, :128] = x_own[0].astype(BF16)
        state[n, place, :, 128:] = x_own[1].astype(BF16)
        for d in (1, 2, 3):
            b = state.at[n, place]
            push(b, b, ss.at[n, d - 1], sr.at[n, d - 1], mates[d - 1])
        for d in (1, 2, 3):
            landed(state.at[n, lax.rem(place - d + 4, 4)], ss.at[n, d - 1], sr.at[n, d - 1])
        total = unpack(state[n, 0].astype(F32))
        before = jnp.zeros_like(total)
        for j in range(1, 4):
            before = jnp.where(place == j, total, before)
            nxt = unpack(state[n, j].astype(F32))
            total = total + nxt + dot(nxt[:, :128], total)
        return total, before

    y_mates = [at(dy=d) for d in (1, 2, 3)]
    t1, b1 = level(0, (e, l), y_mates, y)
    service()
    p1 = pack(t1)
    t2, b2 = level(1, (p1[:, :128], p1[:, 128:]), z_near, zb)
    service()
    p2 = pack(t2)
    _, b3 = level(2, (p2[:, :128], p2[:, 128:]), z_far, za)
    h0 = b3[:, 128:]
    h0 = h0 + dot(b2[:, :128], h0) + b2[:, 128:]
    h0 = h0 + dot(b1[:, :128], h0) + b1[:, 128:]

    o = local_out[...]
    mech = dot(o[:, :128], h0) + o[:, 128:]
    ones = head_ones()
    rf, kf, vf = r_ref[...].astype(F32), k_ref[...].astype(F32), v_ref[...].astype(F32)
    centred = mech - dotx(mech, ones) * (1.0 / 64)
    spread = dotx(centred * centred, ones) * (1.0 / 64)
    token = dotx(rf * kf * stw_ref[...], ones) * vf
    mixed = centred * lax.rsqrt(spread + GROUP_EPS) * hng_ref[...] + token
    mixed = (mixed / (1.0 + jnp.exp(-og_ref[...].astype(F32)))).astype(BF16)

    def shares(a, b, cb):
        for j in range(4):
            cols = D // 4 * j
            bj = b[:, cols : cols + D // 4] if cb == 0 else b[cols : cols + D // 4]
            prod = dot(a, bj, 1, cb)
            for p in range(8):
                part[p // 2, p % 2, :, cols : cols + D // 4] = prod[
                    p * ROWS : (p + 1) * ROWS
                ].astype(BF16)

    def scattered_sum(n):
        other = 1 - core
        for j in range(4):
            push(part.at[j, other], pair_in.at[n, j], ps.at[n, j], pr.at[n, j], at(dc=1))
        for d in (2, 1, 3, 0):
            j = lax.rem(x + d, NX)
            landed(pair_in.at[n, j], ps.at[n, j], pr.at[n, j])
            mine[n, j] = (part[j, core].astype(F32) + pair_in[n, j].astype(F32)).astype(BF16)
            if d:
                push(mine.at[n, j], mix_in.at[n, d - 1], xs.at[n, d - 1], xr.at[n, d - 1], at(dx=d))
        total = mine[n, x].astype(F32)
        for d in (1, 3, 2):
            landed(mix_in.at[n, d - 1], xs.at[n, d - 1], xr.at[n, d - 1])
            total = total + mix_in[n, d - 1].astype(F32)
        return total

    def finish_sends():
        for cp in sends:
            cp.wait_send()
        sends.clear()

    shares(mixed, wo_ref[...], 0)
    service()
    mix = scattered_sum(0).astype(BF16).astype(F32)
    service()
    fetch.wait()
    after = (resid[...].astype(F32) + mix).astype(BF16).astype(F32)
    factor = lax.rsqrt(jnp.mean(after * after, axis=-1, keepdims=True) + NORM_EPS)
    normed = (after * factor * png_ref[...]).astype(BF16)

    rows_buf[x, core] = normed
    mine_rows = rows_buf.at[x, core]
    push(mine_rows, mine_rows, gs.at[0], gr.at[0], at(dc=1))
    for d in (2, 1, 3):
        push(mine_rows, mine_rows, gs.at[d], gr.at[d], at(dx=d))
    for d in (1, 3, 2):
        b = rows_buf.at[lax.rem(x + NX - d, NX), core]
        landed(b, gs.at[d], gr.at[d])
        push(b, b, fs.at[d - 1], fr.at[d - 1], at(dc=1))
    service()
    landed(rows_buf.at[x, 1 - core], gs.at[0], gr.at[0])
    for d in (1, 3, 2):
        b = rows_buf.at[lax.rem(x + NX - d, NX), 1 - core]
        landed(b, fs.at[d - 1], fr.at[d - 1])
    for j in range(8):
        nrm[j * ROWS : (j + 1) * ROWS] = rows_buf[j // 2, j % 2]
    while turn[0] <= 9:
        service()
    finish_sends()

    gate = jnp.zeros((N, FF), F32)
    upper = jnp.zeros((N, FF), F32)
    for j in range(8):
        a = nrm[:, j * 256 : (j + 1) * 256]
        gate = gate + dot(a, gu[j * 8 : (j + 1) * 8, :W].reshape(256, FF))
        upper = upper + dot(a, gu[j * 8 : (j + 1) * 8, W:].reshape(256, FF))
    hidden = (gate / (1.0 + jnp.exp(-gate)) * upper).astype(BF16)
    shares(hidden, dn[...].reshape(D, FF), 1)
    down = scattered_sum(1)
    out_ref[...] = (after + down).astype(BF16)
    finish_sends()


def per_device(r, k, v, dec, lr, og, stw, hng, wo, res, png, wg, wu, wd):
    vmem = pl.BlockSpec(memory_space=pltpu.VMEM)
    hbm = pl.BlockSpec(memory_space=pl.ANY)
    dma = pltpu.SemaphoreType.DMA
    return pl.pallas_call(
        kernel,
        out_shape=jax.ShapeDtypeStruct((ROWS, D), BF16),
        in_specs=[vmem] * 9 + [hbm] + [vmem] + [hbm] * 3,
        out_specs=vmem,
        scratch_shapes=[
            pltpu.VMEM((64, 2 * W, FF), BF16),
            pltpu.VMEM((64, W, FF), BF16),
            pltpu.VMEM((3, 4, 64, 256), BF16),
            pltpu.VMEM((8, 128), F32),
            pltpu.VMEM((NX, NC, ROWS, D), BF16),
            pltpu.VMEM((2, NX, ROWS, D), BF16),
            pltpu.VMEM((2, NX, ROWS, D), BF16),
            pltpu.VMEM((2, 3, ROWS, D), BF16),
            pltpu.VMEM((NX, NC, ROWS, D), BF16),
            pltpu.VMEM((N, D), BF16),
            pltpu.VMEM((N, 256), F32),
            pltpu.VMEM((ROWS, D), BF16),
            dma((4,)),
            dma((2, 8)), dma((2, 8)),
            dma((16, 4)), dma((16, 4)),
            dma((3,)), dma((3,)),
            dma((2, 8)), dma((2, 8)),
            dma((3, 3)), dma((3, 3)),
            dma((2, 4)), dma((2, 4)),
            dma((2, 3)), dma((2, 3)),
            dma((4,)), dma((4,)),
            dma((3,)), dma((3,)),
        ],
        compiler_params=pltpu.CompilerParams(
            collective_id=0, has_side_effects=True, vmem_limit_bytes=60 * 1024 * 1024
        ),
        name="layer",
    )(r, k, v, dec, lr, og, stw.reshape(1, 128), hng.reshape(1, 128), wo, res,
      png.reshape(1, D), wg, wu, wd.T)


def solution(mesh):
    torus = Mesh(mesh.devices.reshape(NZ, NY, NX, NC), ("z", "y", "x", "c"))
    sp, tp = ("z", "y"), ("x", "c")
    seq = P(sp, tp)
    return jax.shard_map(
        per_device,
        mesh=torus,
        in_specs=(
            seq, seq, seq, seq, seq, seq, P(tp, None), P(tp), P(tp, None), P(sp, None), P(),
            seq, seq, P(tp, sp),
        ),
        out_specs=P((*sp, *tp), None),
        check_vma=False,
    )
```

```python
import functools
import math

import jax
import jax.numpy as jnp
from jax import lax
from jax.experimental import pallas as pl
from jax.experimental.pallas import tpu as pltpu
from jax.sharding import Mesh
from jax.sharding import PartitionSpec as P

F32, BF16 = jnp.float32, jnp.bfloat16
EXACT = lax.Precision.HIGHEST
MESH = pl.DeviceIdType.MESH
GROUP_EPS = 0.00064
NORM_EPS = 1e-06

NZ, NY, NX, NC = 16, 4, 4, 2
N = 192
ROWS = 24
D = 2048
FF = 640
W = 32


def dot(a, b, ca=1, cb=0):
    return lax.dot_general(
        a.astype(BF16), b.astype(BF16), (((ca,), (cb,)), ((), ())), preferred_element_type=F32
    )


def dotx(a, b, ca=1, cb=0):
    return lax.dot_general(
        a, b, (((ca,), (cb,)), ((), ())), precision=EXACT, preferred_element_type=F32
    )


def iota(shape, d):
    return lax.broadcasted_iota(jnp.int32, shape, d)


def head_ones():
    return jnp.where(iota((128, 128), 0) // 64 == iota((128, 128), 1) // 64, 1.0, 0.0).astype(F32)


def invert(low):
    n = low.shape[0]
    row, col = iota((n, n), 0), iota((n, n), 1)
    eye = jnp.where(row == col, 1.0, 0.0).astype(F32)
    d = jnp.where(row // 8 == col // 8, low, 0.0)
    d2 = dotx(d, d)
    d4 = dotx(d2, d2)
    x = eye + d
    x = x + dotx(d2, x)
    x = x + dotx(d4, x)
    m = 8
    while m < 64:
        off = jnp.where((row // (2 * m) == col // (2 * m)) & (row // m != col // m), low, 0.0)
        x = x + dot(x, dot(off, x))
        m *= 2
    off = jnp.where(row // 64 != col // 64, low, 0.0)
    y = dot(x, off)
    z = dot(y, x)
    return x + z + dot(y, z)


def local_scan(r, k, v, dec, lr, service):
    r, k, v = r.astype(F32), k.astype(F32), v.astype(F32)
    lw = (-math.exp(-0.5)) / (1.0 + jnp.exp(-dec))
    row, col = iota((N, N), 0), iota((N, N), 1)
    c = dotx(jnp.where(row >= col, 1.0, 0.0).astype(F32), lw)
    norm = jnp.sqrt(dotx(k * k, head_ones()))
    unit = k / jnp.maximum(norm, 1.0)
    ins = unit / (1.0 + jnp.exp(-lr))
    up, dn = jnp.exp(c), jnp.exp(-c)
    last = c[N - 1 : N]
    rest = jnp.exp(last - c)
    at = -unit * jnp.exp(c - lw)
    rt = r * up
    left = jnp.concatenate([at, rt], 0)
    right = jnp.concatenate([ins * dn, k * dn], 0).astype(BF16)
    lane2 = iota((N, 256), 1) % 128
    us, reads = [], []
    for h in range(2):
        head_lanes = iota((2 * N, 128), 1) // 64 == h
        g = dot(jnp.where(head_lanes, left, 0.0), right, 1, 1)
        low = jnp.where(row > col, g[:N, :N], 0.0)
        mak = jnp.where(row > col, g[:N, N:], 0.0)
        mrb = jnp.where(row >= col, g[N:, :N], 0.0)
        mrk = jnp.where(row >= col, g[N:, N:], 0.0)
        x = invert(low)
        u = dot(x, jnp.concatenate([at, dot(mak, v)], 1))
        us.append(u)
        reads.append((mrb, mrk))
        service()
    u = jnp.where(lane2 < 64, us[0], us[1])
    f = dot((ins * rest).T, u)
    fl = f[:, 128:] + dot((k * rest).T, v)
    ones = head_ones()
    r1, c1 = iota((128, 128), 0), iota((128, 128), 1)
    e = f[:, :128] * ones + jnp.where(r1 == c1, jnp.exp(last) - 1.0, 0.0)
    l = fl * ones

    def outputs():
        outs = []
        for h in range(2):
            mrb, mrk = reads[h]
            o = dot(mrb, us[h])
            ov = dot(mrk, v)
            outs.append(jnp.concatenate([o[:, :128] + rt, o[:, 128:] + ov], 1))
        return jnp.where(lane2 < 64, outs[0], outs[1])

    return e[:64] + e[64:], l[:64] + l[64:], outputs


def unpack(p):
    first = iota(p.shape, 1) % 128 < 64
    return jnp.concatenate([jnp.where(first, p, 0.0), jnp.where(first, 0.0, p)], 0)


def pack(p):
    first = iota((64, p.shape[1]), 1) % 128 < 64
    return jnp.where(first, p[:64], p[64:])


def kernel(
    r_ref, k_ref, v_ref, dec_ref, lr_ref, og_ref, stw_ref, hng_ref, wo_ref, res_ref, png_ref,
    wg_ref, wu_ref, wd_ref,
    out_ref,
    gu, dn, state, far, part, pair_in, mine, mix_in, relay, joint, rows_buf, nrm, local_out, resid,
    loc_sem, zs, zr, ys, yr, as_, ar, azs, azr, ss, sr, ps, pr, xs, xr, gs, gr, fs, fr,
):
    z, y, x, core = (lax.axis_index(a) for a in ("z", "y", "x", "c"))
    here = z * NY + y

    def at(dz=0, dy=0, dx=0, dc=0):
        return (
            lax.rem(z + dz + NZ, NZ), lax.rem(y + dy + NY, NY),
            lax.rem(x + dx + NX, NX), lax.rem(core + dc, NC),
        )

    sends = []

    def push(src, dst, send, recv, to):
        cp = pltpu.make_async_remote_copy(
            src_ref=src, dst_ref=dst, send_sem=send, recv_sem=recv, device_id=to,
            device_id_type=MESH,
        )
        cp.start()
        sends.append(cp)
        return cp

    def landed(dst, send, recv):
        pltpu.make_async_remote_copy(
            src_ref=dst, dst_ref=dst, send_sem=send, recv_sem=recv, device_id=at(dz=1),
            device_id_type=MESH,
        ).wait_recv()

    own = [
        pltpu.make_async_copy(wg_ref, gu.at[here, pl.ds(0, W)], loc_sem.at[0]),
        pltpu.make_async_copy(wu_ref, gu.at[here, pl.ds(W, W)], loc_sem.at[1]),
        pltpu.make_async_copy(wd_ref, dn.at[here], loc_sem.at[2]),
    ]
    row0 = pl.multiple_of((x * NC + core) * ROWS, 8)
    fetch = pltpu.make_async_copy(res_ref.at[pl.ds(row0, ROWS)], resid, loc_sem.at[3])
    for cp in own:
        cp.start()
    fetch.start()

    zb, za = z % 4, z // 4
    peers = [at(dz=1), at(dz=-1), at(dy=1), at(dy=2), at(dy=3)]
    peers += [at(dx=d) for d in (1, 2, 3)] + [at(dc=1)]
    z_near = [(za * 4 + lax.rem(zb + d, 4), y, x, core) for d in (1, 2, 3)]
    z_far = [at(dz=4 * d) for d in (1, 2, 3)]
    peers += z_near + z_far
    barrier = pltpu.get_barrier_semaphore()
    for p in peers:
        pl.semaphore_signal(barrier, inc=1, device_id=p, device_id_type=MESH)
    for cp in own:
        cp.wait()
    pl.semaphore_wait(barrier, len(peers))

    def slot(dz, dy=0):
        return lax.rem(z + dz + NZ, NZ) * NY + lax.rem(y + dy + NY, NY)

    def column(dz):
        return pl.multiple_of(lax.rem(z + dz + NZ, NZ) * NY, NY)

    def offsets(s):
        return [0] if s == 0 else ([-s, s] if s < 8 else [8])

    def index(o):
        return 0 if o == 0 else (15 if o == 8 else 2 * abs(o) - (1 if o < 0 else 0))

    def y_out(o):
        i = index(o)
        src = gu.at[slot(o)]
        push(src, src, ys.at[i, 0], yr.at[i, 0], at(dy=1))
        push(src, src, ys.at[i, 1], yr.at[i, 1], at(dy=-1))

    def y_on(o):
        i = index(o)
        a, b = gu.at[slot(o, -1)], gu.at[slot(o, 1)]
        landed(a, ys.at[i, 0], yr.at[i, 0])
        a = gu.at[slot(o, -1), pl.ds(0, W)]
        push(a, a, ys.at[i, 2], yr.at[i, 2], at(dy=1))
        landed(b, ys.at[i, 1], yr.at[i, 1])
        b = gu.at[slot(o, 1), pl.ds(W, W)]
        push(b, b, ys.at[i, 3], yr.at[i, 3], at(dy=-1))

    def y_end(o):
        i = index(o)
        landed(gu.at[slot(o, 2), pl.ds(0, W)], ys.at[i, 2], yr.at[i, 2])
        landed(gu.at[slot(o, 2), pl.ds(W, W)], ys.at[i, 3], yr.at[i, 3])

    def z_block(dz, d, s):
        b = gu.at[slot(dz)]
        return b if s < 8 else gu.at[slot(dz), pl.ds(W * d, W)]

    def z_out(s):
        for d in range(2):
            o = -s if d == 0 else s
            b = z_block(o, d, s + 1)
            push(b, b, zs.at[d, s], zr.at[d, s], at(dz=1 if d == 0 else -1))

    def z_in(s):
        for d in range(2):
            landed(z_block(-s if d == 0 else s, d, s), zs.at[d, s - 1], zr.at[d, s - 1])

    def a_block(dz, d, s):
        return dn.at[pl.ds(column(dz), NY)] if s < 8 else dn.at[pl.ds(column(dz) + 2 * d, 2)]

    def a_out(s):
        for d in range(2):
            b = a_block(-s if d == 0 else s, d, s + 1)
            push(b, b, azs.at[d, s], azr.at[d, s], at(dz=1 if d == 0 else -1))

    def a_in(s):
        for d in range(2):
            b = a_block(-s if d == 0 else s, d, s)
            landed(b, azs.at[d, s - 1], azr.at[d, s - 1])

    turn = [0]

    def service():
        s, weighty = divmod(turn[0], 2)
        turn[0] += 1
        if s == 0 and not weighty:
            z_out(0)
            for d in (1, 3, 2):
                push(dn.at[here], dn.at[here], as_.at[d - 1], ar.at[d - 1], at(dy=d))
            y_out(0)
        elif s <= 8 and not weighty:
            z_in(s)
            if s < 8:
                z_out(s)
            for o in offsets(s):
                y_out(o)
        elif s <= 8:
            if s == 0:
                for d in (1, 2, 3):
                    landed(dn.at[slot(0, -d)], as_.at[d - 1], ar.at[d - 1])
            else:
                a_in(s)
            if s < 8:
                a_out(s)
            if s > 0:
                for o in offsets(s - 1):
                    y_on(o)
        elif s == 9 and not weighty:
            for o in offsets(8):
                y_on(o)
            for t in range(9):
                for o in offsets(t):
                    y_end(o)

    service()

    e, l, outputs = local_scan(
        r_ref[...], k_ref[...], v_ref[...], dec_ref[...], lr_ref[...], service
    )

    def level(n, x_own, mates, place, meanwhile):
        state[n, place, :, :128] = x_own[0].astype(BF16)
        state[n, place, :, 128:] = x_own[1].astype(BF16)
        for d in (2, 1, 3):
            b = state.at[n, place]
            push(b, b, ss.at[n, d - 1], sr.at[n, d - 1], mates[d - 1])
        meanwhile()
        for d in (1, 3, 2):
            landed(state.at[n, lax.rem(place - d + 4, 4)], ss.at[n, d - 1], sr.at[n, d - 1])
        total = unpack(state[n, 0].astype(F32))
        before = jnp.zeros_like(total)
        for j in range(1, 4):
            before = jnp.where(place == j, total, before)
            nxt = unpack(state[n, j].astype(F32))
            total = total + nxt + dot(nxt[:, :128], total)
        return total, before

    def meanwhile_outputs():
        local_out[...] = outputs()
        service()

    def meanwhile_services():
        service()
        service()

    y_mates = [at(dy=d) for d in (1, 2, 3)]
    t1, b1 = level(0, (e, l), y_mates, y, meanwhile_outputs)
    p1 = pack(t1)
    t2, b2 = level(1, (p1[:, :128], p1[:, 128:]), z_near, zb, meanwhile_services)

    p2 = pack(t2).astype(BF16)
    quarter = jnp.zeros((16, 256), BF16)
    for j in range(4):
        quarter = jnp.where(y == j, p2[j * 16 : (j + 1) * 16], quarter)
    far[za, y] = quarter
    for d in (2, 1, 3):
        b = far.at[za, y]
        push(b, b, ss.at[2, d - 1], sr.at[2, d - 1], z_far[d - 1])
    service()
    service()
    for d in (1, 3, 2):
        landed(far.at[lax.rem(za - d + 4, 4), y], ss.at[2, d - 1], sr.at[2, d - 1])
    for d in (2, 1, 3):
        b = far.at[:, y]
        push(b, b, ss.at[3, d - 1], sr.at[3, d - 1], y_mates[d - 1])
    service()
    for d in (1, 3, 2):
        landed(far.at[:, lax.rem(y - d + 4, 4)], ss.at[3, d - 1], sr.at[3, d - 1])
    total = unpack(far[0].reshape(64, 256)[:, 128:].astype(F32))
    h0 = jnp.zeros_like(total)
    for j in range(1, 4):
        h0 = jnp.where(za == j, total, h0)
        if j < 3:
            nxt = unpack(far[j].reshape(64, 256).astype(F32))
            total = total + nxt[:, 128:] + dot(nxt[:, :128], total)
    h0 = h0 + dot(b2[:, :128], h0) + b2[:, 128:]
    h0 = h0 + dot(b1[:, :128], h0) + b1[:, 128:]

    o = local_out[...]
    mech = dot(o[:, :128], h0) + o[:, 128:]
    ones = head_ones()
    rf, kf, vf = r_ref[...].astype(F32), k_ref[...].astype(F32), v_ref[...].astype(F32)
    centred = mech - dotx(mech, ones) * (1.0 / 64)
    spread = dotx(centred * centred, ones) * (1.0 / 64)
    token = dotx(rf * kf * stw_ref[...], ones) * vf
    mixed = centred * lax.rsqrt(spread + GROUP_EPS) * hng_ref[...] + token
    mixed = (mixed / (1.0 + jnp.exp(-og_ref[...].astype(F32)))).astype(BF16)

    def shares(a, b, cb):
        for j in range(4):
            cols = D // 4 * j
            bj = b[:, cols : cols + D // 4] if cb == 0 else b[cols : cols + D // 4]
            prod = dot(a, bj, 1, cb)
            for p in range(8):
                part[p // 2, p % 2, :, cols : cols + D // 4] = prod[
                    p * ROWS : (p + 1) * ROWS
                ].astype(BF16)

    halves = (pl.ds(0, D // 2), pl.ds(D // 2, D // 2))

    def scattered_sum(n, meanwhile):
        other = 1 - core
        across = lax.rem(x + 2, NX)
        sides = (lax.rem(x + 1, NX), lax.rem(x + 3, NX))
        steps = (at(dx=1), at(dx=-1))
        order = (across, *sides, x)
        for i, j in enumerate(order):
            push(part.at[j, other], pair_in.at[n, j], ps.at[n, i], pr.at[n, i], at(dc=1))
        for i, j in enumerate(order):
            landed(pair_in.at[n, j], ps.at[n, i], pr.at[n, i])
            mine[n, j] = (part[j, core].astype(F32) + pair_in[n, j].astype(F32)).astype(BF16)
            if i == 0:
                for e in range(2):
                    push(mine.at[n, j, :, halves[e]], relay.at[n, e], xs.at[n, e], xr.at[n, e], steps[e])
            elif i < 3:
                cut = halves[2 - i]
                push(
                    mine.at[n, j, :, cut], mix_in.at[n, i - 1, :, cut], xs.at[n, 1 + i],
                    xr.at[n, 1 + i], steps[i - 1],
                )
        meanwhile()
        for e in range(2):
            landed(relay.at[n, e], xs.at[n, e], xr.at[n, e])
            joint[n, e] = (
                mine[n, sides[e], :, halves[e]].astype(F32) + relay[n, e].astype(F32)
            ).astype(BF16)
            push(
                joint.at[n, e], mix_in.at[n, e, :, halves[e]], xs.at[n, 4 + e], xr.at[n, 4 + e],
                steps[e],
            )
        meanwhile()
        total = mine[n, x].astype(F32)
        for e in range(2):
            landed(mix_in.at[n, e, :, halves[1 - e]], xs.at[n, 2 + e], xr.at[n, 2 + e])
            landed(mix_in.at[n, e, :, halves[e]], xs.at[n, 4 + e], xr.at[n, 4 + e])
            total = total + mix_in[n, e].astype(F32)
        return total

    def finish_sends():
        for cp in sends:
            cp.wait_send()
        sends.clear()

    shares(mixed, wo_ref[...], 0)
    mix = scattered_sum(0, service).astype(BF16).astype(F32)
    fetch.wait()
    after = (resid[...].astype(F32) + mix).astype(BF16).astype(F32)
    factor = lax.rsqrt(jnp.mean(after * after, axis=-1, keepdims=True) + NORM_EPS)
    normed = (after * factor * png_ref[...]).astype(BF16)

    rows_buf[x, core] = normed
    mine_rows = rows_buf.at[x, core]
    for e in range(2):
        b = rows_buf.at[x, core, :, halves[e]]
        push(b, b, gs.at[e, 0], gr.at[e, 0], at(dx=1 if e == 0 else -1))
    for e in range(2):
        b = rows_buf.at[x, core, :, halves[1 - e]]
        push(b, b, gs.at[e, 1], gr.at[e, 1], at(dx=1 if e == 0 else -1))
    push(mine_rows, mine_rows, fs.at[0], fr.at[0], at(dc=1))
    service()

    def came(dx, e, half, i, k, onward):
        b = rows_buf.at[lax.rem(x + dx, NX), core, :, halves[half]]
        landed(b, gs.at[e, i], gr.at[e, i])
        if onward:
            push(b, b, gs.at[e, 2], gr.at[e, 2], at(dx=1 if e == 0 else -1))
        push(b, b, fs.at[k], fr.at[k], at(dc=1))

    came(3, 0, 0, 0, 1, True)
    came(1, 1, 1, 0, 2, True)
    came(3, 0, 1, 1, 3, False)
    came(1, 1, 0, 1, 4, False)
    service()
    came(2, 0, 0, 2, 5, False)
    came(2, 1, 1, 2, 6, False)
    landed(rows_buf.at[x, 1 - core], fs.at[0], fr.at[0])
    for k, (dx, half) in enumerate(((3, 0), (1, 1), (3, 1), (1, 0), (2, 0), (2, 1))):
        b = rows_buf.at[lax.rem(x + dx, NX), 1 - core, :, halves[half]]
        landed(b, fs.at[k + 1], fr.at[k + 1])
    for j in range(8):
        nrm[j * ROWS : (j + 1) * ROWS] = rows_buf[j // 2, j % 2]
    while turn[0] <= 18:
        service()
    finish_sends()

    gate = jnp.zeros((N, FF), F32)
    upper = jnp.zeros((N, FF), F32)
    for j in range(8):
        a = nrm[:, j * 256 : (j + 1) * 256]
        gate = gate + dot(a, gu[j * 8 : (j + 1) * 8, :W].reshape(256, FF))
        upper = upper + dot(a, gu[j * 8 : (j + 1) * 8, W:].reshape(256, FF))
    hidden = (gate / (1.0 + jnp.exp(-gate)) * upper).astype(BF16)
    shares(hidden, dn[...].reshape(D, FF), 1)
    down = scattered_sum(1, lambda: None)
    out_ref[...] = (after + down).astype(BF16)
    finish_sends()


def per_device(r, k, v, dec, lr, og, stw, hng, wo, res, png, wg, wu, wd):
    vmem = pl.BlockSpec(memory_space=pltpu.VMEM)
    hbm = pl.BlockSpec(memory_space=pl.ANY)
    dma = pltpu.SemaphoreType.DMA
    return pl.pallas_call(
        kernel,
        out_shape=jax.ShapeDtypeStruct((ROWS, D), BF16),
        in_specs=[vmem] * 9 + [hbm] + [vmem] + [hbm] * 3,
        out_specs=vmem,
        scratch_shapes=[
            pltpu.VMEM((64, 2 * W, FF), BF16),
            pltpu.VMEM((64, W, FF), BF16),
            pltpu.VMEM((2, 4, 64, 256), BF16),
            pltpu.VMEM((4, NY, 16, 256), BF16),
            pltpu.VMEM((NX, NC, ROWS, D), BF16),
            pltpu.VMEM((2, NX, ROWS, D), BF16),
            pltpu.VMEM((2, NX, ROWS, D), BF16),
            pltpu.VMEM((2, 2, ROWS, D), BF16),
            pltpu.VMEM((2, 2, ROWS, D // 2), BF16),
            pltpu.VMEM((2, 2, ROWS, D // 2), BF16),
            pltpu.VMEM((NX, NC, ROWS, D), BF16),
            pltpu.VMEM((N, D), BF16),
            pltpu.VMEM((N, 256), F32),
            pltpu.VMEM((ROWS, D), BF16),
            dma((4,)),
            dma((2, 8)), dma((2, 8)),
            dma((16, 4)), dma((16, 4)),
            dma((3,)), dma((3,)),
            dma((2, 8)), dma((2, 8)),
            dma((4, 3)), dma((4, 3)),
            dma((2, 4)), dma((2, 4)),
            dma((2, 6)), dma((2, 6)),
            dma((2, 3)), dma((2, 3)),
            dma((7,)), dma((7,)),
        ],
        compiler_params=pltpu.CompilerParams(
            collective_id=0, has_side_effects=True, vmem_limit_bytes=60 * 1024 * 1024
        ),
        name="layer",
    )(r, k, v, dec, lr, og, stw.reshape(1, 128), hng.reshape(1, 128), wo, res,
      png.reshape(1, D), wg, wu, wd.T)


def solution(mesh):
    torus = Mesh(mesh.devices.reshape(NZ, NY, NX, NC), ("z", "y", "x", "c"))
    sp, tp = ("z", "y"), ("x", "c")
    seq = P(sp, tp)
    return jax.shard_map(
        per_device,
        mesh=torus,
        in_specs=(
            seq, seq, seq, seq, seq, seq, P(tp, None), P(tp), P(tp, None), P(sp, None), P(),
            seq, seq, P(tp, sp),
        ),
        out_specs=P((*sp, *tp), None),
        check_vma=False,
    )
```

```python
import functools
import math

import jax
import jax.numpy as jnp
from jax import lax
from jax.experimental import pallas as pl
from jax.experimental.pallas import tpu as pltpu
from jax.sharding import Mesh
from jax.sharding import PartitionSpec as P

F32, BF16 = jnp.float32, jnp.bfloat16
EXACT = lax.Precision.HIGHEST
MESH = pl.DeviceIdType.MESH
GROUP_EPS = 0.00064
NORM_EPS = 1e-06

NZ, NY, NX, NC = 16, 4, 4, 2
N = 192
ROWS = 24
D = 2048
FF = 640
W = 32
TURNS = 28
POINTS = 19


def dot(a, b, ca=1, cb=0):
    return lax.dot_general(
        a.astype(BF16), b.astype(BF16), (((ca,), (cb,)), ((), ())), preferred_element_type=F32
    )


def dotx(a, b, ca=1, cb=0):
    return lax.dot_general(
        a, b, (((ca,), (cb,)), ((), ())), precision=EXACT, preferred_element_type=F32
    )


def iota(shape, d):
    return lax.broadcasted_iota(jnp.int32, shape, d)


def head_ones():
    return jnp.where(iota((128, 128), 0) // 64 == iota((128, 128), 1) // 64, 1.0, 0.0).astype(F32)


def invert(low):
    n = low.shape[0]
    row, col = iota((n, n), 0), iota((n, n), 1)
    eye = jnp.where(row == col, 1.0, 0.0).astype(F32)
    d = jnp.where(row // 8 == col // 8, low, 0.0)
    d2 = dotx(d, d)
    d4 = dotx(d2, d2)
    x = eye + d
    x = x + dotx(d2, x)
    x = x + dotx(d4, x)
    m = 8
    while m < 64:
        off = jnp.where((row // (2 * m) == col // (2 * m)) & (row // m != col // m), low, 0.0)
        x = x + dot(x, dot(off, x))
        m *= 2
    off = jnp.where(row // 64 != col // 64, low, 0.0)
    y = dot(x, off)
    z = dot(y, x)
    return x + z + dot(y, z)


def local_scan(r, k, v, dec, lr, service):
    r, k, v = r.astype(F32), k.astype(F32), v.astype(F32)
    lw = (-math.exp(-0.5)) / (1.0 + jnp.exp(-dec))
    row, col = iota((N, N), 0), iota((N, N), 1)
    c = dotx(jnp.where(row >= col, 1.0, 0.0).astype(F32), lw)
    norm = jnp.sqrt(dotx(k * k, head_ones()))
    unit = k / jnp.maximum(norm, 1.0)
    ins = unit / (1.0 + jnp.exp(-lr))
    up, dn = jnp.exp(c), jnp.exp(-c)
    last = c[N - 1 : N]
    rest = jnp.exp(last - c)
    at = -unit * jnp.exp(c - lw)
    rt = r * up
    left = jnp.concatenate([at, rt], 0)
    right = jnp.concatenate([ins * dn, k * dn], 0).astype(BF16)
    lane2 = iota((N, 256), 1) % 128
    us, reads = [], []
    for h in range(2):
        head_lanes = iota((2 * N, 128), 1) // 64 == h
        g = dot(jnp.where(head_lanes, left, 0.0), right, 1, 1)
        low = jnp.where(row > col, g[:N, :N], 0.0)
        mak = jnp.where(row > col, g[:N, N:], 0.0)
        mrb = jnp.where(row >= col, g[N:, :N], 0.0)
        mrk = jnp.where(row >= col, g[N:, N:], 0.0)
        x = invert(low)
        service()
        u = dot(x, jnp.concatenate([at, dot(mak, v)], 1))
        us.append(u)
        reads.append((mrb, mrk))
        if h == 1:
            service()
    u = jnp.where(lane2 < 64, us[0], us[1])
    f = dot((ins * rest).T, u)
    fl = f[:, 128:] + dot((k * rest).T, v)
    ones = head_ones()
    r1, c1 = iota((128, 128), 0), iota((128, 128), 1)
    e = f[:, :128] * ones + jnp.where(r1 == c1, jnp.exp(last) - 1.0, 0.0)
    l = fl * ones

    def outputs():
        outs = []
        for h in range(2):
            mrb, mrk = reads[h]
            o = dot(mrb, us[h])
            ov = dot(mrk, v)
            outs.append(jnp.concatenate([o[:, :128] + rt, o[:, 128:] + ov], 1))
        return jnp.where(lane2 < 64, outs[0], outs[1])

    return e[:64] + e[64:], l[:64] + l[64:], outputs


def unpack(p):
    first = iota(p.shape, 1) % 128 < 64
    return jnp.concatenate([jnp.where(first, p, 0.0), jnp.where(first, 0.0, p)], 0)


def pack(p):
    first = iota((64, p.shape[1]), 1) % 128 < 64
    return jnp.where(first, p[:64], p[64:])


def kernel(
    r_ref, k_ref, v_ref, dec_ref, lr_ref, og_ref, stw_ref, hng_ref, wo_ref, res_ref, png_ref,
    wg_ref, wu_ref, wd_ref,
    out_ref,
    gu, dn, state, far, part, pair_in, mine, mix_in, relay, joint, rows_buf, nrm, local_out, resid,
    loc_sem, zs, zr, ys, yr, as_, ar, azs, azr, ss, sr, ps, pr, xs, xr, gs, gr, fs, fr,
):
    z, y, x, core = (lax.axis_index(a) for a in ("z", "y", "x", "c"))
    here = z * NY + y

    def at(dz=0, dy=0, dx=0, dc=0):
        return (
            lax.rem(z + dz + NZ, NZ), lax.rem(y + dy + NY, NY),
            lax.rem(x + dx + NX, NX), lax.rem(core + dc, NC),
        )

    sends = []

    def push(src, dst, send, recv, to):
        cp = pltpu.make_async_remote_copy(
            src_ref=src, dst_ref=dst, send_sem=send, recv_sem=recv, device_id=to,
            device_id_type=MESH,
        )
        cp.start()
        sends.append(cp)
        return cp

    def landed(dst, send, recv):
        pltpu.make_async_remote_copy(
            src_ref=dst, dst_ref=dst, send_sem=send, recv_sem=recv, device_id=at(dz=1),
            device_id_type=MESH,
        ).wait_recv()

    own = [
        pltpu.make_async_copy(wg_ref, gu.at[here, pl.ds(0, W)], loc_sem.at[0]),
        pltpu.make_async_copy(wu_ref, gu.at[here, pl.ds(W, W)], loc_sem.at[1]),
        pltpu.make_async_copy(wd_ref, dn.at[here], loc_sem.at[2]),
    ]
    row0 = pl.multiple_of((x * NC + core) * ROWS, 8)
    fetch = pltpu.make_async_copy(res_ref.at[pl.ds(row0, ROWS)], resid, loc_sem.at[3])
    for cp in own:
        cp.start()
    fetch.start()

    zb, za = z % 4, z // 4
    peers = [at(dz=1), at(dz=-1), at(dy=1), at(dy=2), at(dy=3)]
    peers += [at(dx=d) for d in (1, 2, 3)] + [at(dc=1)]
    z_near = [(za * 4 + lax.rem(zb + d, 4), y, x, core) for d in (1, 2, 3)]
    z_far = [at(dz=4 * d) for d in (1, 2, 3)]
    peers += z_near + z_far
    barrier = pltpu.get_barrier_semaphore()
    for p in peers:
        pl.semaphore_signal(barrier, inc=1, device_id=p, device_id_type=MESH)
    for cp in own:
        cp.wait()
    pl.semaphore_wait(barrier, len(peers))

    def slot(dz, dy=0):
        return lax.rem(z + dz + NZ, NZ) * NY + lax.rem(y + dy + NY, NY)

    def column(dz):
        return pl.multiple_of(lax.rem(z + dz + NZ, NZ) * NY, NY)

    def offsets(s):
        return [0] if s == 0 else ([-s, s] if s < 8 else [8])

    def index(o):
        return 0 if o == 0 else (15 if o == 8 else 2 * abs(o) - (1 if o < 0 else 0))

    def y_out(o):
        i = index(o)
        src = gu.at[slot(o)]
        push(src, src, ys.at[i, 0], yr.at[i, 0], at(dy=1))
        push(src, src, ys.at[i, 1], yr.at[i, 1], at(dy=-1))

    def y_on(o):
        i = index(o)
        a, b = gu.at[slot(o, -1)], gu.at[slot(o, 1)]
        landed(a, ys.at[i, 0], yr.at[i, 0])
        a = gu.at[slot(o, -1), pl.ds(0, W)]
        push(a, a, ys.at[i, 2], yr.at[i, 2], at(dy=1))
        landed(b, ys.at[i, 1], yr.at[i, 1])
        b = gu.at[slot(o, 1), pl.ds(W, W)]
        push(b, b, ys.at[i, 3], yr.at[i, 3], at(dy=-1))

    def y_end(o):
        i = index(o)
        landed(gu.at[slot(o, 2), pl.ds(0, W)], ys.at[i, 2], yr.at[i, 2])
        landed(gu.at[slot(o, 2), pl.ds(W, W)], ys.at[i, 3], yr.at[i, 3])

    def z_block(dz, d, s):
        b = gu.at[slot(dz)]
        return b if s < 8 else gu.at[slot(dz), pl.ds(W * d, W)]

    def z_out(s):
        for d in range(2):
            o = -s if d == 0 else s
            b = z_block(o, d, s + 1)
            push(b, b, zs.at[d, s], zr.at[d, s], at(dz=1 if d == 0 else -1))

    def z_in(s):
        for d in range(2):
            landed(z_block(-s if d == 0 else s, d, s), zs.at[d, s - 1], zr.at[d, s - 1])

    def a_dirs(s, g):
        return (0, 1) if s < 8 else (g,)

    def a_block(s, d, g):
        return dn.at[pl.ds(column(-s if d == 0 else s) + 2 * g, 2)]

    def a_out(s, g):
        for d in a_dirs(s + 1, g):
            b = a_block(s, d, g)
            push(b, b, azs.at[d, g, s], azr.at[d, g, s], at(dz=1 if d == 0 else -1))

    def a_in(s, g):
        for d in a_dirs(s, g):
            landed(a_block(s, d, g), azs.at[d, g, s - 1], azr.at[d, g, s - 1])

    turn, points = [0], [0]

    def service():
        points[0] += 1
        while turn[0] < min(points[0] * TURNS // POINTS, TURNS):
            one_turn()

    def one_turn():
        s, g = divmod(turn[0], 3)
        turn[0] += 1
        if s == 0 and g == 0:
            z_out(0)
            for d in (1, 3, 2):
                push(dn.at[here], dn.at[here], as_.at[d - 1], ar.at[d - 1], at(dy=d))
            y_out(0)
        elif s <= 8 and g == 0:
            z_in(s)
            if s < 8:
                z_out(s)
            for o in offsets(s):
                y_out(o)
        elif s <= 8:
            if s == 0 and g == 1:
                for d in (1, 2, 3):
                    landed(dn.at[slot(0, -d)], as_.at[d - 1], ar.at[d - 1])
            if s > 0:
                a_in(s, g - 1)
            if s < 8:
                a_out(s, g - 1)
            if s > 0:
                for o in offsets(s - 1)[g - 1 : g]:
                    y_on(o)
        else:
            for o in offsets(8):
                y_on(o)
            for t in range(9):
                for o in offsets(t):
                    y_end(o)

    service()

    e, l, outputs = local_scan(
        r_ref[...], k_ref[...], v_ref[...], dec_ref[...], lr_ref[...], service
    )

    def level(n, x_own, mates, place, meanwhile):
        state[n, place, :, :128] = x_own[0].astype(BF16)
        state[n, place, :, 128:] = x_own[1].astype(BF16)
        for d in (2, 1, 3):
            b = state.at[n, place]
            push(b, b, ss.at[n, d - 1], sr.at[n, d - 1], mates[d - 1])
        meanwhile()
        for d in (1, 3, 2):
            landed(state.at[n, lax.rem(place - d + 4, 4)], ss.at[n, d - 1], sr.at[n, d - 1])
        total = unpack(state[n, 0].astype(F32))
        before = jnp.zeros_like(total)
        for j in range(1, 4):
            before = jnp.where(place == j, total, before)
            nxt = unpack(state[n, j].astype(F32))
            total = total + nxt + dot(nxt[:, :128], total)
        return total, before

    def meanwhile_outputs():
        service()
        local_out[...] = outputs()
        service()

    def meanwhile_services():
        service()
        service()

    y_mates = [at(dy=d) for d in (1, 2, 3)]
    t1, b1 = level(0, (e, l), y_mates, y, meanwhile_outputs)
    p1 = pack(t1)
    t2, b2 = level(1, (p1[:, :128], p1[:, 128:]), z_near, zb, meanwhile_services)

    p2 = pack(t2).astype(BF16)
    quarter = jnp.zeros((16, 256), BF16)
    for j in range(4):
        quarter = jnp.where(y == j, p2[j * 16 : (j + 1) * 16], quarter)
    far[za, y] = quarter
    for d in (2, 1, 3):
        b = far.at[za, y]
        push(b, b, ss.at[2, d - 1], sr.at[2, d - 1], z_far[d - 1])
    service()
    service()
    for d in (1, 3, 2):
        landed(far.at[lax.rem(za - d + 4, 4), y], ss.at[2, d - 1], sr.at[2, d - 1])
    for d in (2, 1, 3):
        b = far.at[:, y]
        push(b, b, ss.at[3, d - 1], sr.at[3, d - 1], y_mates[d - 1])
    service()
    for d in (1, 3, 2):
        landed(far.at[:, lax.rem(y - d + 4, 4)], ss.at[3, d - 1], sr.at[3, d - 1])
    total = unpack(far[0].reshape(64, 256)[:, 128:].astype(F32))
    h0 = jnp.zeros_like(total)
    for j in range(1, 4):
        h0 = jnp.where(za == j, total, h0)
        if j < 3:
            nxt = unpack(far[j].reshape(64, 256).astype(F32))
            total = total + nxt[:, 128:] + dot(nxt[:, :128], total)
    h0 = h0 + dot(b2[:, :128], h0) + b2[:, 128:]
    h0 = h0 + dot(b1[:, :128], h0) + b1[:, 128:]

    o = local_out[...]
    mech = dot(o[:, :128], h0) + o[:, 128:]
    ones = head_ones()
    rf, kf, vf = r_ref[...].astype(F32), k_ref[...].astype(F32), v_ref[...].astype(F32)
    centred = mech - dotx(mech, ones) * (1.0 / 64)
    spread = dotx(centred * centred, ones) * (1.0 / 64)
    token = dotx(rf * kf * stw_ref[...], ones) * vf
    mixed = centred * lax.rsqrt(spread + GROUP_EPS) * hng_ref[...] + token
    mixed = (mixed / (1.0 + jnp.exp(-og_ref[...].astype(F32)))).astype(BF16)

    def shares(a, b, cb):
        for j in range(4):
            cols = D // 4 * j
            bj = b[:, cols : cols + D // 4] if cb == 0 else b[cols : cols + D // 4]
            prod = dot(a, bj, 1, cb)
            for p in range(8):
                part[p // 2, p % 2, :, cols : cols + D // 4] = prod[
                    p * ROWS : (p + 1) * ROWS
                ].astype(BF16)

    halves = (pl.ds(0, D // 2), pl.ds(D // 2, D // 2))

    def scattered_sum(n, meanwhile):
        other = 1 - core
        across = lax.rem(x + 2, NX)
        sides = (lax.rem(x + 1, NX), lax.rem(x + 3, NX))
        steps = (at(dx=1), at(dx=-1))
        order = (across, *sides, x)
        for i, j in enumerate(order):
            push(part.at[j, other], pair_in.at[n, j], ps.at[n, i], pr.at[n, i], at(dc=1))
        meanwhile()
        for i, j in enumerate(order):
            landed(pair_in.at[n, j], ps.at[n, i], pr.at[n, i])
            mine[n, j] = (part[j, core].astype(F32) + pair_in[n, j].astype(F32)).astype(BF16)
            if i == 0:
                for e in range(2):
                    push(mine.at[n, j, :, halves[e]], relay.at[n, e], xs.at[n, e], xr.at[n, e], steps[e])
            elif i < 3:
                cut = halves[2 - i]
                push(
                    mine.at[n, j, :, cut], mix_in.at[n, i - 1, :, cut], xs.at[n, 1 + i],
                    xr.at[n, 1 + i], steps[i - 1],
                )
        meanwhile()
        for e in range(2):
            landed(relay.at[n, e], xs.at[n, e], xr.at[n, e])
            joint[n, e] = (
                mine[n, sides[e], :, halves[e]].astype(F32) + relay[n, e].astype(F32)
            ).astype(BF16)
            push(
                joint.at[n, e], mix_in.at[n, e, :, halves[e]], xs.at[n, 4 + e], xr.at[n, 4 + e],
                steps[e],
            )
        meanwhile()
        total = mine[n, x].astype(F32)
        for e in range(2):
            landed(mix_in.at[n, e, :, halves[1 - e]], xs.at[n, 2 + e], xr.at[n, 2 + e])
            landed(mix_in.at[n, e, :, halves[e]], xs.at[n, 4 + e], xr.at[n, 4 + e])
            total = total + mix_in[n, e].astype(F32)
        return total

    def finish_sends():
        for cp in sends:
            cp.wait_send()
        sends.clear()

    service()
    shares(mixed, wo_ref[...], 0)
    mix = scattered_sum(0, service).astype(BF16).astype(F32)
    fetch.wait()
    after = (resid[...].astype(F32) + mix).astype(BF16).astype(F32)
    factor = lax.rsqrt(jnp.mean(after * after, axis=-1, keepdims=True) + NORM_EPS)
    normed = (after * factor * png_ref[...]).astype(BF16)

    rows_buf[x, core] = normed
    mine_rows = rows_buf.at[x, core]
    for e in range(2):
        b = rows_buf.at[x, core, :, halves[e]]
        push(b, b, gs.at[e, 0], gr.at[e, 0], at(dx=1 if e == 0 else -1))
    for e in range(2):
        b = rows_buf.at[x, core, :, halves[1 - e]]
        push(b, b, gs.at[e, 1], gr.at[e, 1], at(dx=1 if e == 0 else -1))
    push(mine_rows, mine_rows, fs.at[0], fr.at[0], at(dc=1))
    service()
    service()

    def came(dx, e, half, i, k, onward):
        b = rows_buf.at[lax.rem(x + dx, NX), core, :, halves[half]]
        landed(b, gs.at[e, i], gr.at[e, i])
        if onward:
            push(b, b, gs.at[e, 2], gr.at[e, 2], at(dx=1 if e == 0 else -1))
        push(b, b, fs.at[k], fr.at[k], at(dc=1))

    came(3, 0, 0, 0, 1, True)
    came(1, 1, 1, 0, 2, True)
    came(3, 0, 1, 1, 3, False)
    came(1, 1, 0, 1, 4, False)
    service()
    came(2, 0, 0, 2, 5, False)
    came(2, 1, 1, 2, 6, False)
    landed(rows_buf.at[x, 1 - core], fs.at[0], fr.at[0])
    for k, (dx, half) in enumerate(((3, 0), (1, 1), (3, 1), (1, 0), (2, 0), (2, 1))):
        b = rows_buf.at[lax.rem(x + dx, NX), 1 - core, :, halves[half]]
        landed(b, fs.at[k + 1], fr.at[k + 1])
    for j in range(8):
        nrm[j * ROWS : (j + 1) * ROWS] = rows_buf[j // 2, j % 2]
    while turn[0] < TURNS:
        one_turn()
    finish_sends()

    gate = jnp.zeros((N, FF), F32)
    upper = jnp.zeros((N, FF), F32)
    for j in range(8):
        a = nrm[:, j * 256 : (j + 1) * 256]
        gate = gate + dot(a, gu[j * 8 : (j + 1) * 8, :W].reshape(256, FF))
        upper = upper + dot(a, gu[j * 8 : (j + 1) * 8, W:].reshape(256, FF))
    hidden = (gate / (1.0 + jnp.exp(-gate)) * upper).astype(BF16)
    shares(hidden, dn[...].reshape(D, FF), 1)
    down = scattered_sum(1, lambda: None)
    out_ref[...] = (after + down).astype(BF16)
    finish_sends()


def per_device(r, k, v, dec, lr, og, stw, hng, wo, res, png, wg, wu, wd):
    vmem = pl.BlockSpec(memory_space=pltpu.VMEM)
    hbm = pl.BlockSpec(memory_space=pl.ANY)
    dma = pltpu.SemaphoreType.DMA
    return pl.pallas_call(
        kernel,
        out_shape=jax.ShapeDtypeStruct((ROWS, D), BF16),
        in_specs=[vmem] * 9 + [hbm] + [vmem] + [hbm] * 3,
        out_specs=vmem,
        scratch_shapes=[
            pltpu.VMEM((64, 2 * W, FF), BF16),
            pltpu.VMEM((64, W, FF), BF16),
            pltpu.VMEM((2, 4, 64, 256), BF16),
            pltpu.VMEM((4, NY, 16, 256), BF16),
            pltpu.VMEM((NX, NC, ROWS, D), BF16),
            pltpu.VMEM((2, NX, ROWS, D), BF16),
            pltpu.VMEM((2, NX, ROWS, D), BF16),
            pltpu.VMEM((2, 2, ROWS, D), BF16),
            pltpu.VMEM((2, 2, ROWS, D // 2), BF16),
            pltpu.VMEM((2, 2, ROWS, D // 2), BF16),
            pltpu.VMEM((NX, NC, ROWS, D), BF16),
            pltpu.VMEM((N, D), BF16),
            pltpu.VMEM((N, 256), F32),
            pltpu.VMEM((ROWS, D), BF16),
            dma((4,)),
            dma((2, 8)), dma((2, 8)),
            dma((16, 4)), dma((16, 4)),
            dma((3,)), dma((3,)),
            dma((2, 2, 8)), dma((2, 2, 8)),
            dma((4, 3)), dma((4, 3)),
            dma((2, 4)), dma((2, 4)),
            dma((2, 6)), dma((2, 6)),
            dma((2, 3)), dma((2, 3)),
            dma((7,)), dma((7,)),
        ],
        compiler_params=pltpu.CompilerParams(
            collective_id=0, has_side_effects=True, vmem_limit_bytes=60 * 1024 * 1024
        ),
        name="layer",
    )(r, k, v, dec, lr, og, stw.reshape(1, 128), hng.reshape(1, 128), wo, res,
      png.reshape(1, D), wg, wu, wd.T)


def solution(mesh):
    torus = Mesh(mesh.devices.reshape(NZ, NY, NX, NC), ("z", "y", "x", "c"))
    sp, tp = ("z", "y"), ("x", "c")
    seq = P(sp, tp)
    return jax.shard_map(
        per_device,
        mesh=torus,
        in_specs=(
            seq, seq, seq, seq, seq, seq, P(tp, None), P(tp), P(tp, None), P(sp, None), P(),
            seq, seq, P(tp, sp),
        ),
        out_specs=P((*sp, *tp), None),
        check_vma=False,
    )
```

```python
import functools
import math

import jax
import jax.numpy as jnp
from jax import lax
from jax.experimental import pallas as pl
from jax.experimental.pallas import tpu as pltpu
from jax.sharding import Mesh
from jax.sharding import PartitionSpec as P

F32, BF16 = jnp.float32, jnp.bfloat16
EXACT = lax.Precision.HIGHEST
MESH = pl.DeviceIdType.MESH
GROUP_EPS = 0.00064
NORM_EPS = 1e-06

NZ, NY, NX, NC = 16, 4, 4, 2
N = 192
ROWS = 24
D = 2048
FF = 640
W = 32
TURNS = 28
POINTS = 19


def dot(a, b, ca=1, cb=0):
    return lax.dot_general(
        a.astype(BF16), b.astype(BF16), (((ca,), (cb,)), ((), ())), preferred_element_type=F32
    )


def dotx(a, b, ca=1, cb=0):
    return lax.dot_general(
        a, b, (((ca,), (cb,)), ((), ())), precision=EXACT, preferred_element_type=F32
    )


def iota(shape, d):
    return lax.broadcasted_iota(jnp.int32, shape, d)


def head_ones():
    return jnp.where(iota((128, 128), 0) // 64 == iota((128, 128), 1) // 64, 1.0, 0.0).astype(F32)


def invert(low):
    n = low.shape[0]
    row, col = iota((n, n), 0), iota((n, n), 1)
    eye = jnp.where(row == col, 1.0, 0.0).astype(F32)
    d = jnp.where(row // 8 == col // 8, low, 0.0)
    d2 = dotx(d, d)
    d4 = dotx(d2, d2)
    x = eye + d
    x = x + dotx(d2, x)
    x = x + dotx(d4, x)
    m = 8
    while m < 64:
        off = jnp.where((row // (2 * m) == col // (2 * m)) & (row // m != col // m), low, 0.0)
        x = x + dot(x, dot(off, x))
        m *= 2
    off = jnp.where(row // 64 != col // 64, low, 0.0)
    y = dot(x, off)
    z = dot(y, x)
    return x + z + dot(y, z)


def local_scan(r, k, v, dec, lr, service):
    r, k, v = r.astype(F32), k.astype(F32), v.astype(F32)
    lw = (-math.exp(-0.5)) / (1.0 + jnp.exp(-dec))
    row, col = iota((N, N), 0), iota((N, N), 1)
    c = dotx(jnp.where(row >= col, 1.0, 0.0).astype(F32), lw)
    norm = jnp.sqrt(dotx(k * k, head_ones()))
    unit = k / jnp.maximum(norm, 1.0)
    ins = unit / (1.0 + jnp.exp(-lr))
    up, dn = jnp.exp(c), jnp.exp(-c)
    last = c[N - 1 : N]
    rest = jnp.exp(last - c)
    at = -unit * jnp.exp(c - lw)
    rt = r * up
    left = jnp.concatenate([at, rt], 0)
    right = jnp.concatenate([ins * dn, k * dn], 0).astype(BF16)
    lane2 = iota((N, 256), 1) % 128
    us, reads = [], []
    for h in range(2):
        head_lanes = iota((2 * N, 128), 1) // 64 == h
        g = dot(jnp.where(head_lanes, left, 0.0), right, 1, 1)
        low = jnp.where(row > col, g[:N, :N], 0.0)
        mak = jnp.where(row > col, g[:N, N:], 0.0)
        mrb = jnp.where(row >= col, g[N:, :N], 0.0)
        mrk = jnp.where(row >= col, g[N:, N:], 0.0)
        x = invert(low)
        service()
        u = dot(x, jnp.concatenate([at, dot(mak, v)], 1))
        us.append(u)
        reads.append((mrb, mrk))
        if h == 1:
            service()
    u = jnp.where(lane2 < 64, us[0], us[1])
    f = dot((ins * rest).T, u)
    fl = f[:, 128:] + dot((k * rest).T, v)
    ones = head_ones()
    r1, c1 = iota((128, 128), 0), iota((128, 128), 1)
    e = f[:, :128] * ones + jnp.where(r1 == c1, jnp.exp(last) - 1.0, 0.0)
    l = fl * ones

    def outputs():
        outs = []
        for h in range(2):
            mrb, mrk = reads[h]
            o = dot(mrb, us[h])
            ov = dot(mrk, v)
            outs.append(jnp.concatenate([o[:, :128] + rt, o[:, 128:] + ov], 1))
        return jnp.where(lane2 < 64, outs[0], outs[1])

    return e[:64] + e[64:], l[:64] + l[64:], outputs


def unpack(p):
    first = iota(p.shape, 1) % 128 < 64
    return jnp.concatenate([jnp.where(first, p, 0.0), jnp.where(first, 0.0, p)], 0)


def pack(p):
    first = iota((64, p.shape[1]), 1) % 128 < 64
    return jnp.where(first, p[:64], p[64:])


def kernel(
    r_ref, k_ref, v_ref, dec_ref, lr_ref, og_ref, stw_ref, hng_ref, wo_ref, res_ref, png_ref,
    wg_ref, wu_ref, wd_ref,
    out_ref,
    gu, dn, state, far, part, pair_in, mine, mix_in, relay, joint, rows_buf, nrm, local_out, resid,
    loc_sem, word, zs, zr, ys, yr, as_, ar, azs, azr, ss, sr, ps, pr, xs, xr, gs, gr, fs, fr,
):
    z, y, x, core = (lax.axis_index(a) for a in ("z", "y", "x", "c"))
    here = z * NY + y

    def at(dz=0, dy=0, dx=0, dc=0):
        return (
            lax.rem(z + dz + NZ, NZ), lax.rem(y + dy + NY, NY),
            lax.rem(x + dx + NX, NX), lax.rem(core + dc, NC),
        )

    sends = []

    def push(src, dst, send, recv, to):
        cp = pltpu.make_async_remote_copy(
            src_ref=src, dst_ref=dst, send_sem=send, recv_sem=recv, device_id=to,
            device_id_type=MESH,
        )
        cp.start()
        sends.append(cp)
        return cp

    def landed(dst, send, recv):
        pltpu.make_async_remote_copy(
            src_ref=dst, dst_ref=dst, send_sem=send, recv_sem=recv, device_id=at(dz=1),
            device_id_type=MESH,
        ).wait_recv()

    own = [
        pltpu.make_async_copy(wg_ref, gu.at[here, pl.ds(0, W)], loc_sem.at[0]),
        pltpu.make_async_copy(wu_ref, gu.at[here, pl.ds(W, W)], loc_sem.at[1]),
        pltpu.make_async_copy(wd_ref, dn.at[here], loc_sem.at[2]),
    ]
    row0 = pl.multiple_of((x * NC + core) * ROWS, 8)
    fetch = pltpu.make_async_copy(res_ref.at[pl.ds(row0, ROWS)], resid, loc_sem.at[3])
    for cp in own:
        cp.start()
    fetch.start()

    zb, za = z % 4, z // 4
    peers = [at(dz=1), at(dz=-1), at(dy=1), at(dy=2), at(dy=3)]
    peers += [at(dx=1), at(dx=-1), at(dc=1)]
    z_near = [(za * 4 + lax.rem(zb + d, 4), y, x, core) for d in (1, 2, 3)]
    z_far = [at(dz=4 * d) for d in (1, 2, 3)]
    barrier = pltpu.get_barrier_semaphore()
    for p in peers:
        pl.semaphore_signal(barrier, inc=1, device_id=p, device_id_type=MESH)
    for cp in own:
        cp.wait()
    pl.semaphore_wait(barrier, len(peers))

    def word_on(t):
        for d in range(2):
            to = at(dz=1 if d == 0 else -1)
            pl.semaphore_signal(word.at[d, t], inc=1, device_id=to, device_id_type=MESH)

    def word_in(t):
        for d in range(2):
            pl.semaphore_wait(word.at[d, t], 1)

    word_on(0)

    def slot(dz, dy=0):
        return lax.rem(z + dz + NZ, NZ) * NY + lax.rem(y + dy + NY, NY)

    def column(dz):
        return pl.multiple_of(lax.rem(z + dz + NZ, NZ) * NY, NY)

    def offsets(s):
        return [0] if s == 0 else ([-s, s] if s < 8 else [8])

    def index(o):
        return 0 if o == 0 else (15 if o == 8 else 2 * abs(o) - (1 if o < 0 else 0))

    def y_out(o):
        i = index(o)
        src = gu.at[slot(o)]
        push(src, src, ys.at[i, 0], yr.at[i, 0], at(dy=1))
        push(src, src, ys.at[i, 1], yr.at[i, 1], at(dy=-1))

    def y_on(o):
        i = index(o)
        a, b = gu.at[slot(o, -1)], gu.at[slot(o, 1)]
        landed(a, ys.at[i, 0], yr.at[i, 0])
        a = gu.at[slot(o, -1), pl.ds(0, W)]
        push(a, a, ys.at[i, 2], yr.at[i, 2], at(dy=1))
        landed(b, ys.at[i, 1], yr.at[i, 1])
        b = gu.at[slot(o, 1), pl.ds(W, W)]
        push(b, b, ys.at[i, 3], yr.at[i, 3], at(dy=-1))

    def y_end(o):
        i = index(o)
        landed(gu.at[slot(o, 2), pl.ds(0, W)], ys.at[i, 2], yr.at[i, 2])
        landed(gu.at[slot(o, 2), pl.ds(W, W)], ys.at[i, 3], yr.at[i, 3])

    def z_block(dz, d, s):
        b = gu.at[slot(dz)]
        return b if s < 8 else gu.at[slot(dz), pl.ds(W * d, W)]

    def z_out(s):
        for d in range(2):
            o = -s if d == 0 else s
            b = z_block(o, d, s + 1)
            push(b, b, zs.at[d, s], zr.at[d, s], at(dz=1 if d == 0 else -1))

    def z_in(s):
        for d in range(2):
            landed(z_block(-s if d == 0 else s, d, s), zs.at[d, s - 1], zr.at[d, s - 1])

    def a_dirs(s, g):
        return (0, 1) if s < 8 else (g,)

    def a_block(s, d, g):
        return dn.at[pl.ds(column(-s if d == 0 else s) + 2 * g, 2)]

    def a_out(s, g):
        for d in a_dirs(s + 1, g):
            b = a_block(s, d, g)
            push(b, b, azs.at[d, g, s], azr.at[d, g, s], at(dz=1 if d == 0 else -1))

    def a_in(s, g):
        for d in a_dirs(s, g):
            landed(a_block(s, d, g), azs.at[d, g, s - 1], azr.at[d, g, s - 1])

    turn, points = [0], [0]

    def service():
        points[0] += 1
        while turn[0] < min(points[0] * TURNS // POINTS, TURNS):
            one_turn()

    def one_turn():
        s, g = divmod(turn[0], 3)
        turn[0] += 1
        if 2 <= turn[0] <= 8:
            word_in(turn[0] - 2)
            if turn[0] < 8:
                word_on(turn[0] - 1)
        if s == 0 and g == 0:
            z_out(0)
            for d in (1, 3, 2):
                push(dn.at[here], dn.at[here], as_.at[d - 1], ar.at[d - 1], at(dy=d))
            y_out(0)
        elif s <= 8 and g == 0:
            z_in(s)
            if s < 8:
                z_out(s)
            for o in offsets(s):
                y_out(o)
        elif s <= 8:
            if s == 0 and g == 1:
                for d in (1, 2, 3):
                    landed(dn.at[slot(0, -d)], as_.at[d - 1], ar.at[d - 1])
            if s > 0:
                a_in(s, g - 1)
            if s < 8:
                a_out(s, g - 1)
            if s > 0:
                for o in offsets(s - 1)[g - 1 : g]:
                    y_on(o)
        else:
            for o in offsets(8):
                y_on(o)
            for t in range(9):
                for o in offsets(t):
                    y_end(o)

    service()

    e, l, outputs = local_scan(
        r_ref[...], k_ref[...], v_ref[...], dec_ref[...], lr_ref[...], service
    )

    def level(n, x_own, mates, place, meanwhile):
        state[n, place, :, :128] = x_own[0].astype(BF16)
        state[n, place, :, 128:] = x_own[1].astype(BF16)
        for d in (2, 1, 3):
            b = state.at[n, place]
            push(b, b, ss.at[n, d - 1], sr.at[n, d - 1], mates[d - 1])
        meanwhile()
        for d in (1, 3, 2):
            landed(state.at[n, lax.rem(place - d + 4, 4)], ss.at[n, d - 1], sr.at[n, d - 1])
        total = unpack(state[n, 0].astype(F32))
        before = jnp.zeros_like(total)
        for j in range(1, 4):
            before = jnp.where(place == j, total, before)
            nxt = unpack(state[n, j].astype(F32))
            total = total + nxt + dot(nxt[:, :128], total)
        return total, before

    def meanwhile_outputs():
        service()
        local_out[...] = outputs()
        service()

    def meanwhile_services():
        service()
        service()

    y_mates = [at(dy=d) for d in (1, 2, 3)]
    t1, b1 = level(0, (e, l), y_mates, y, meanwhile_outputs)
    p1 = pack(t1)
    t2, b2 = level(1, (p1[:, :128], p1[:, 128:]), z_near, zb, meanwhile_services)

    p2 = pack(t2).astype(BF16)
    quarter = jnp.zeros((16, 256), BF16)
    for j in range(4):
        quarter = jnp.where(y == j, p2[j * 16 : (j + 1) * 16], quarter)
    far[za, y] = quarter
    for d in (2, 1, 3):
        b = far.at[za, y]
        push(b, b, ss.at[2, d - 1], sr.at[2, d - 1], z_far[d - 1])
    service()
    service()
    for d in (1, 3, 2):
        landed(far.at[lax.rem(za - d + 4, 4), y], ss.at[2, d - 1], sr.at[2, d - 1])
    for d in (2, 1, 3):
        b = far.at[:, y]
        push(b, b, ss.at[3, d - 1], sr.at[3, d - 1], y_mates[d - 1])
    service()
    for d in (1, 3, 2):
        landed(far.at[:, lax.rem(y - d + 4, 4)], ss.at[3, d - 1], sr.at[3, d - 1])
    total = unpack(far[0].reshape(64, 256)[:, 128:].astype(F32))
    h0 = jnp.zeros_like(total)
    for j in range(1, 4):
        h0 = jnp.where(za == j, total, h0)
        if j < 3:
            nxt = unpack(far[j].reshape(64, 256).astype(F32))
            total = total + nxt[:, 128:] + dot(nxt[:, :128], total)
    h0 = h0 + dot(b2[:, :128], h0) + b2[:, 128:]
    h0 = h0 + dot(b1[:, :128], h0) + b1[:, 128:]

    o = local_out[...]
    mech = dot(o[:, :128], h0) + o[:, 128:]
    ones = head_ones()
    rf, kf, vf = r_ref[...].astype(F32), k_ref[...].astype(F32), v_ref[...].astype(F32)
    centred = mech - dotx(mech, ones) * (1.0 / 64)
    spread = dotx(centred * centred, ones) * (1.0 / 64)
    token = dotx(rf * kf * stw_ref[...], ones) * vf
    mixed = centred * lax.rsqrt(spread + GROUP_EPS) * hng_ref[...] + token
    mixed = (mixed / (1.0 + jnp.exp(-og_ref[...].astype(F32)))).astype(BF16)

    def shares(a, b, cb):
        for j in range(4):
            cols = D // 4 * j
            bj = b[:, cols : cols + D // 4] if cb == 0 else b[cols : cols + D // 4]
            prod = dot(a, bj, 1, cb)
            for p in range(8):
                part[p // 2, p % 2, :, cols : cols + D // 4] = prod[
                    p * ROWS : (p + 1) * ROWS
                ].astype(BF16)

    halves = (pl.ds(0, D // 2), pl.ds(D // 2, D // 2))

    def scattered_sum(n, meanwhile):
        other = 1 - core
        across = lax.rem(x + 2, NX)
        sides = (lax.rem(x + 1, NX), lax.rem(x + 3, NX))
        steps = (at(dx=1), at(dx=-1))
        order = (across, *sides, x)
        for i, j in enumerate(order):
            push(part.at[j, other], pair_in.at[n, j], ps.at[n, i], pr.at[n, i], at(dc=1))
        meanwhile()
        for i, j in enumerate(order):
            landed(pair_in.at[n, j], ps.at[n, i], pr.at[n, i])
            mine[n, j] = (part[j, core].astype(F32) + pair_in[n, j].astype(F32)).astype(BF16)
            if i == 0:
                for e in range(2):
                    push(mine.at[n, j, :, halves[e]], relay.at[n, e], xs.at[n, e], xr.at[n, e], steps[e])
            elif i < 3:
                cut = halves[2 - i]
                push(
                    mine.at[n, j, :, cut], mix_in.at[n, i - 1, :, cut], xs.at[n, 1 + i],
                    xr.at[n, 1 + i], steps[i - 1],
                )
        meanwhile()
        for e in range(2):
            landed(relay.at[n, e], xs.at[n, e], xr.at[n, e])
            joint[n, e] = (
                mine[n, sides[e], :, halves[e]].astype(F32) + relay[n, e].astype(F32)
            ).astype(BF16)
            push(
                joint.at[n, e], mix_in.at[n, e, :, halves[e]], xs.at[n, 4 + e], xr.at[n, 4 + e],
                steps[e],
            )
        meanwhile()
        total = mine[n, x].astype(F32)
        for e in range(2):
            landed(mix_in.at[n, e, :, halves[1 - e]], xs.at[n, 2 + e], xr.at[n, 2 + e])
            landed(mix_in.at[n, e, :, halves[e]], xs.at[n, 4 + e], xr.at[n, 4 + e])
            total = total + mix_in[n, e].astype(F32)
        return total

    def finish_sends():
        for cp in sends:
            cp.wait_send()
        sends.clear()

    service()
    shares(mixed, wo_ref[...], 0)
    mix = scattered_sum(0, service).astype(BF16).astype(F32)
    fetch.wait()
    after = (resid[...].astype(F32) + mix).astype(BF16).astype(F32)
    factor = lax.rsqrt(jnp.mean(after * after, axis=-1, keepdims=True) + NORM_EPS)
    normed = (after * factor * png_ref[...]).astype(BF16)

    rows_buf[x, core] = normed
    mine_rows = rows_buf.at[x, core]
    for e in range(2):
        b = rows_buf.at[x, core, :, halves[e]]
        push(b, b, gs.at[e, 0], gr.at[e, 0], at(dx=1 if e == 0 else -1))
    for e in range(2):
        b = rows_buf.at[x, core, :, halves[1 - e]]
        push(b, b, gs.at[e, 1], gr.at[e, 1], at(dx=1 if e == 0 else -1))
    push(mine_rows, mine_rows, fs.at[0], fr.at[0], at(dc=1))
    service()
    service()

    def came(dx, e, half, i, k, onward):
        b = rows_buf.at[lax.rem(x + dx, NX), core, :, halves[half]]
        landed(b, gs.at[e, i], gr.at[e, i])
        if onward:
            push(b, b, gs.at[e, 2], gr.at[e, 2], at(dx=1 if e == 0 else -1))
        push(b, b, fs.at[k], fr.at[k], at(dc=1))

    came(3, 0, 0, 0, 1, True)
    came(1, 1, 1, 0, 2, True)
    came(3, 0, 1, 1, 3, False)
    came(1, 1, 0, 1, 4, False)
    service()
    came(2, 0, 0, 2, 5, False)
    came(2, 1, 1, 2, 6, False)
    landed(rows_buf.at[x, 1 - core], fs.at[0], fr.at[0])
    for k, (dx, half) in enumerate(((3, 0), (1, 1), (3, 1), (1, 0), (2, 0), (2, 1))):
        b = rows_buf.at[lax.rem(x + dx, NX), 1 - core, :, halves[half]]
        landed(b, fs.at[k + 1], fr.at[k + 1])
    for j in range(8):
        nrm[j * ROWS : (j + 1) * ROWS] = rows_buf[j // 2, j % 2]
    while turn[0] < TURNS:
        one_turn()
    finish_sends()

    gate = jnp.zeros((N, FF), F32)
    upper = jnp.zeros((N, FF), F32)
    for j in range(8):
        a = nrm[:, j * 256 : (j + 1) * 256]
        gate = gate + dot(a, gu[j * 8 : (j + 1) * 8, :W].reshape(256, FF))
        upper = upper + dot(a, gu[j * 8 : (j + 1) * 8, W:].reshape(256, FF))
    hidden = (gate / (1.0 + jnp.exp(-gate)) * upper).astype(BF16)
    shares(hidden, dn[...].reshape(D, FF), 1)
    down = scattered_sum(1, lambda: None)
    out_ref[...] = (after + down).astype(BF16)
    finish_sends()


def per_device(r, k, v, dec, lr, og, stw, hng, wo, res, png, wg, wu, wd):
    vmem = pl.BlockSpec(memory_space=pltpu.VMEM)
    hbm = pl.BlockSpec(memory_space=pl.ANY)
    dma = pltpu.SemaphoreType.DMA
    return pl.pallas_call(
        kernel,
        out_shape=jax.ShapeDtypeStruct((ROWS, D), BF16),
        in_specs=[vmem] * 9 + [hbm] + [vmem] + [hbm] * 3,
        out_specs=vmem,
        scratch_shapes=[
            pltpu.VMEM((64, 2 * W, FF), BF16),
            pltpu.VMEM((64, W, FF), BF16),
            pltpu.VMEM((2, 4, 64, 256), BF16),
            pltpu.VMEM((4, NY, 16, 256), BF16),
            pltpu.VMEM((NX, NC, ROWS, D), BF16),
            pltpu.VMEM((2, NX, ROWS, D), BF16),
            pltpu.VMEM((2, NX, ROWS, D), BF16),
            pltpu.VMEM((2, 2, ROWS, D), BF16),
            pltpu.VMEM((2, 2, ROWS, D // 2), BF16),
            pltpu.VMEM((2, 2, ROWS, D // 2), BF16),
            pltpu.VMEM((NX, NC, ROWS, D), BF16),
            pltpu.VMEM((N, D), BF16),
            pltpu.VMEM((N, 256), F32),
            pltpu.VMEM((ROWS, D), BF16),
            dma((4,)), pltpu.SemaphoreType.REGULAR((2, 7)),
            dma((2, 8)), dma((2, 8)),
            dma((16, 4)), dma((16, 4)),
            dma((3,)), dma((3,)),
            dma((2, 2, 8)), dma((2, 2, 8)),
            dma((4, 3)), dma((4, 3)),
            dma((2, 4)), dma((2, 4)),
            dma((2, 6)), dma((2, 6)),
            dma((2, 3)), dma((2, 3)),
            dma((7,)), dma((7,)),
        ],
        compiler_params=pltpu.CompilerParams(
            collective_id=0, has_side_effects=True, vmem_limit_bytes=60 * 1024 * 1024
        ),
        name="layer",
    )(r, k, v, dec, lr, og, stw.reshape(1, 128), hng.reshape(1, 128), wo, res,
      png.reshape(1, D), wg, wu, wd.T)


def solution(mesh):
    torus = Mesh(mesh.devices.reshape(NZ, NY, NX, NC), ("z", "y", "x", "c"))
    sp, tp = ("z", "y"), ("x", "c")
    seq = P(sp, tp)
    return jax.shard_map(
        per_device,
        mesh=torus,
        in_specs=(
            seq, seq, seq, seq, seq, seq, P(tp, None), P(tp), P(tp, None), P(sp, None), P(),
            seq, seq, P(tp, sp),
        ),
        out_specs=P((*sp, *tp), None),
        check_vma=False,
    )
```

```python
import functools
import math

import jax
import jax.numpy as jnp
from jax import lax
from jax.experimental import pallas as pl
from jax.experimental.pallas import tpu as pltpu
from jax.sharding import Mesh
from jax.sharding import PartitionSpec as P

F32, BF16 = jnp.float32, jnp.bfloat16
EXACT = lax.Precision.HIGHEST
MESH = pl.DeviceIdType.MESH
GROUP_EPS = 0.00064
NORM_EPS = 1e-06

NZ, NY, NX, NC = 16, 4, 4, 2
N = 192
ROWS = 24
D = 2048
FF = 640
W = 32
TURNS = 28
POINTS = 19


def dot(a, b, ca=1, cb=0):
    return lax.dot_general(
        a.astype(BF16), b.astype(BF16), (((ca,), (cb,)), ((), ())), preferred_element_type=F32
    )


def dotx(a, b, ca=1, cb=0):
    return lax.dot_general(
        a, b, (((ca,), (cb,)), ((), ())), precision=EXACT, preferred_element_type=F32
    )


def iota(shape, d):
    return lax.broadcasted_iota(jnp.int32, shape, d)


def head_ones():
    return jnp.where(iota((128, 128), 0) // 64 == iota((128, 128), 1) // 64, 1.0, 0.0).astype(F32)


def invert(low):
    n = low.shape[0]
    row, col = iota((n, n), 0), iota((n, n), 1)
    eye = jnp.where(row == col, 1.0, 0.0).astype(F32)
    d = jnp.where(row // 8 == col // 8, low, 0.0)
    d2 = dotx(d, d)
    d4 = dotx(d2, d2)
    x = eye + d
    x = x + dotx(d2, x)
    x = x + dotx(d4, x)
    m = 8
    while m < 64:
        off = jnp.where((row // (2 * m) == col // (2 * m)) & (row // m != col // m), low, 0.0)
        x = x + dot(x, dot(off, x))
        m *= 2
    off = jnp.where(row // 64 != col // 64, low, 0.0)
    y = dot(x, off)
    z = dot(y, x)
    return x + z + dot(y, z)


def local_scan(r, k, v, dec, lr, service):
    r, k, v = r.astype(F32), k.astype(F32), v.astype(F32)
    lw = (-math.exp(-0.5)) / (1.0 + jnp.exp(-dec))
    row, col = iota((N, N), 0), iota((N, N), 1)
    c = dotx(jnp.where(row >= col, 1.0, 0.0).astype(F32), lw)
    norm = jnp.sqrt(dotx(k * k, head_ones()))
    unit = k / jnp.maximum(norm, 1.0)
    ins = unit / (1.0 + jnp.exp(-lr))
    up, dn = jnp.exp(c), jnp.exp(-c)
    last = c[N - 1 : N]
    rest = jnp.exp(last - c)
    at = -unit * jnp.exp(c - lw)
    rt = r * up
    left = jnp.concatenate([at, rt], 0)
    right = jnp.concatenate([ins * dn, k * dn], 0).astype(BF16)
    lane2 = iota((N, 256), 1) % 128
    us, reads = [], []
    for h in range(2):
        head_lanes = iota((2 * N, 128), 1) // 64 == h
        g = dot(jnp.where(head_lanes, left, 0.0), right, 1, 1)
        low = jnp.where(row > col, g[:N, :N], 0.0)
        mak = jnp.where(row > col, g[:N, N:], 0.0)
        mrb = jnp.where(row >= col, g[N:, :N], 0.0)
        mrk = jnp.where(row >= col, g[N:, N:], 0.0)
        x = invert(low)
        service()
        u = dot(x, jnp.concatenate([at, dot(mak, v)], 1))
        us.append(u)
        reads.append((mrb, mrk))
        if h == 1:
            service()
    u = jnp.where(lane2 < 64, us[0], us[1])
    f = dot((ins * rest).T, u)
    fl = f[:, 128:] + dot((k * rest).T, v)
    ones = head_ones()
    r1, c1 = iota((128, 128), 0), iota((128, 128), 1)
    e = f[:, :128] * ones + jnp.where(r1 == c1, jnp.exp(last) - 1.0, 0.0)
    l = fl * ones

    def outputs():
        outs = []
        for h in range(2):
            mrb, mrk = reads[h]
            o = dot(mrb, us[h])
            ov = dot(mrk, v)
            outs.append(jnp.concatenate([o[:, :128] + rt, o[:, 128:] + ov], 1))
        return jnp.where(lane2 < 64, outs[0], outs[1])

    return e[:64] + e[64:], l[:64] + l[64:], outputs


def unpack(p):
    first = iota(p.shape, 1) % 128 < 64
    return jnp.concatenate([jnp.where(first, p, 0.0), jnp.where(first, 0.0, p)], 0)


def pack(p):
    first = iota((64, p.shape[1]), 1) % 128 < 64
    return jnp.where(first, p[:64], p[64:])


def kernel(
    r_in, k_in, v_in, dec_in, lr_in, og_in, stw_in, hng_in, wo_in, res_ref, png_in,
    wg_ref, wu_ref, wd_ref,
    out_ref,
    r_ref, k_ref, v_ref, dec_ref, lr_ref, og_ref, stw_ref, hng_ref, wo_ref, png_ref,
    gu, dn, state, far, part, pair_in, mine, mix_in, relay, joint, rows_buf, nrm, local_out, resid,
    loc_sem, in_sem, word, zs, zr, ys, yr, as_, ar, azs, azr, ss, sr, ps, pr, xs, xr, gs, gr, fs, fr,
):
    z, y, x, core = (lax.axis_index(a) for a in ("z", "y", "x", "c"))
    here = z * NY + y

    def at(dz=0, dy=0, dx=0, dc=0):
        return (
            lax.rem(z + dz + NZ, NZ), lax.rem(y + dy + NY, NY),
            lax.rem(x + dx + NX, NX), lax.rem(core + dc, NC),
        )

    sends = []

    def push(src, dst, send, recv, to):
        cp = pltpu.make_async_remote_copy(
            src_ref=src, dst_ref=dst, send_sem=send, recv_sem=recv, device_id=to,
            device_id_type=MESH,
        )
        cp.start()
        sends.append(cp)
        return cp

    def landed(dst, send, recv):
        pltpu.make_async_remote_copy(
            src_ref=dst, dst_ref=dst, send_sem=send, recv_sem=recv, device_id=at(dz=1),
            device_id_type=MESH,
        ).wait_recv()

    own = [
        pltpu.make_async_copy(wg_ref, gu.at[here, pl.ds(0, W)], loc_sem.at[0]),
        pltpu.make_async_copy(wu_ref, gu.at[here, pl.ds(W, W)], loc_sem.at[1]),
        pltpu.make_async_copy(wd_ref, dn.at[here], loc_sem.at[2]),
    ]
    row0 = pl.multiple_of((x * NC + core) * ROWS, 8)
    fetch = pltpu.make_async_copy(res_ref.at[pl.ds(row0, ROWS)], resid, loc_sem.at[3])

    zb, za = z % 4, z // 4
    peers = [at(dz=1), at(dz=-1), at(dy=1), at(dy=2), at(dy=3)]
    peers += [at(dx=1), at(dx=-1), at(dc=1)]
    z_near = [(za * 4 + lax.rem(zb + d, 4), y, x, core) for d in (1, 2, 3)]
    z_far = [at(dz=4 * d) for d in (1, 2, 3)]
    barrier = pltpu.get_barrier_semaphore()
    for p in peers:
        pl.semaphore_signal(barrier, inc=1, device_id=p, device_id_type=MESH)
    pairs = (
        (r_in, r_ref), (k_in, k_ref), (v_in, v_ref), (dec_in, dec_ref), (lr_in, lr_ref),
        (og_in, og_ref), (stw_in, stw_ref), (hng_in, hng_ref), (wo_in, wo_ref), (png_in, png_ref),
    )
    staged = [pltpu.make_async_copy(a, b, in_sem.at[i]) for i, (a, b) in enumerate(pairs)]
    for cp in (*own, *staged, fetch):
        cp.start()
    for cp in own:
        cp.wait()
    pl.semaphore_wait(barrier, len(peers))

    def word_on(t):
        for d in range(2):
            to = at(dz=1 if d == 0 else -1)
            pl.semaphore_signal(word.at[d, t], inc=1, device_id=to, device_id_type=MESH)

    def word_in(t):
        for d in range(2):
            pl.semaphore_wait(word.at[d, t], 1)

    word_on(0)

    def slot(dz, dy=0):
        return lax.rem(z + dz + NZ, NZ) * NY + lax.rem(y + dy + NY, NY)

    def column(dz):
        return pl.multiple_of(lax.rem(z + dz + NZ, NZ) * NY, NY)

    def offsets(s):
        return [0] if s == 0 else ([-s, s] if s < 8 else [8])

    def index(o):
        return 0 if o == 0 else (15 if o == 8 else 2 * abs(o) - (1 if o < 0 else 0))

    def y_out(o):
        i = index(o)
        src = gu.at[slot(o)]
        push(src, src, ys.at[i, 0], yr.at[i, 0], at(dy=1))
        push(src, src, ys.at[i, 1], yr.at[i, 1], at(dy=-1))

    def y_on(o):
        i = index(o)
        a, b = gu.at[slot(o, -1)], gu.at[slot(o, 1)]
        landed(a, ys.at[i, 0], yr.at[i, 0])
        a = gu.at[slot(o, -1), pl.ds(0, W)]
        push(a, a, ys.at[i, 2], yr.at[i, 2], at(dy=1))
        landed(b, ys.at[i, 1], yr.at[i, 1])
        b = gu.at[slot(o, 1), pl.ds(W, W)]
        push(b, b, ys.at[i, 3], yr.at[i, 3], at(dy=-1))

    def y_end(o):
        i = index(o)
        landed(gu.at[slot(o, 2), pl.ds(0, W)], ys.at[i, 2], yr.at[i, 2])
        landed(gu.at[slot(o, 2), pl.ds(W, W)], ys.at[i, 3], yr.at[i, 3])

    def z_block(dz, d, s):
        b = gu.at[slot(dz)]
        return b if s < 8 else gu.at[slot(dz), pl.ds(W * d, W)]

    def z_out(s):
        for d in range(2):
            o = -s if d == 0 else s
            b = z_block(o, d, s + 1)
            push(b, b, zs.at[d, s], zr.at[d, s], at(dz=1 if d == 0 else -1))

    def z_in(s):
        for d in range(2):
            landed(z_block(-s if d == 0 else s, d, s), zs.at[d, s - 1], zr.at[d, s - 1])

    def a_dirs(s, g):
        return (0, 1) if s < 8 else (g,)

    def a_block(s, d, g):
        return dn.at[pl.ds(column(-s if d == 0 else s) + 2 * g, 2)]

    def a_out(s, g):
        for d in a_dirs(s + 1, g):
            b = a_block(s, d, g)
            push(b, b, azs.at[d, g, s], azr.at[d, g, s], at(dz=1 if d == 0 else -1))

    def a_in(s, g):
        for d in a_dirs(s, g):
            landed(a_block(s, d, g), azs.at[d, g, s - 1], azr.at[d, g, s - 1])

    turn, points = [0], [0]

    def service():
        points[0] += 1
        while turn[0] < min(points[0] * TURNS // POINTS, TURNS):
            one_turn()

    def one_turn():
        s, g = divmod(turn[0], 3)
        turn[0] += 1
        if 2 <= turn[0] <= 8:
            word_in(turn[0] - 2)
            if turn[0] < 8:
                word_on(turn[0] - 1)
        if s == 0 and g == 0:
            z_out(0)
            for d in (1, 3, 2):
                push(dn.at[here], dn.at[here], as_.at[d - 1], ar.at[d - 1], at(dy=d))
            y_out(0)
        elif s <= 8 and g == 0:
            z_in(s)
            if s < 8:
                z_out(s)
            for o in offsets(s):
                y_out(o)
        elif s <= 8:
            if s == 0 and g == 1:
                for d in (1, 2, 3):
                    landed(dn.at[slot(0, -d)], as_.at[d - 1], ar.at[d - 1])
            if s > 0:
                a_in(s, g - 1)
            if s < 8:
                a_out(s, g - 1)
            if s > 0:
                for o in offsets(s - 1)[g - 1 : g]:
                    y_on(o)
        else:
            for o in offsets(8):
                y_on(o)

    service()

    for cp in staged[:5]:
        cp.wait()

    e, l, outputs = local_scan(
        r_ref[...], k_ref[...], v_ref[...], dec_ref[...], lr_ref[...], service
    )

    def level(n, x_own, mates, place, meanwhile):
        state[n, place, :, :128] = x_own[0].astype(BF16)
        state[n, place, :, 128:] = x_own[1].astype(BF16)
        for d in (2, 1, 3):
            b = state.at[n, place]
            push(b, b, ss.at[n, d - 1], sr.at[n, d - 1], mates[d - 1])
        meanwhile()
        for d in (1, 3, 2):
            landed(state.at[n, lax.rem(place - d + 4, 4)], ss.at[n, d - 1], sr.at[n, d - 1])
        total = unpack(state[n, 0].astype(F32))
        before = jnp.zeros_like(total)
        for j in range(1, 4):
            before = jnp.where(place == j, total, before)
            nxt = unpack(state[n, j].astype(F32))
            total = total + nxt + dot(nxt[:, :128], total)
        return total, before

    def meanwhile_outputs():
        service()
        local_out[...] = outputs()
        service()

    def meanwhile_services():
        service()
        service()

    y_mates = [at(dy=d) for d in (1, 2, 3)]
    t1, b1 = level(0, (e, l), y_mates, y, meanwhile_outputs)
    p1 = pack(t1)
    t2, b2 = level(1, (p1[:, :128], p1[:, 128:]), z_near, zb, meanwhile_services)

    p2 = pack(t2).astype(BF16)
    quarter = jnp.zeros((16, 256), BF16)
    for j in range(4):
        quarter = jnp.where(y == j, p2[j * 16 : (j + 1) * 16], quarter)
    far[za, y] = quarter
    for d in (2, 1, 3):
        b = far.at[za, y]
        push(b, b, ss.at[2, d - 1], sr.at[2, d - 1], z_far[d - 1])
    service()
    service()
    for d in (1, 3, 2):
        landed(far.at[lax.rem(za - d + 4, 4), y], ss.at[2, d - 1], sr.at[2, d - 1])
    for d in (2, 1, 3):
        b = far.at[:, y]
        push(b, b, ss.at[3, d - 1], sr.at[3, d - 1], y_mates[d - 1])
    service()
    for d in (1, 3, 2):
        landed(far.at[:, lax.rem(y - d + 4, 4)], ss.at[3, d - 1], sr.at[3, d - 1])
    total = unpack(far[0].reshape(64, 256)[:, 128:].astype(F32))
    h0 = jnp.zeros_like(total)
    for j in range(1, 4):
        h0 = jnp.where(za == j, total, h0)
        if j < 3:
            nxt = unpack(far[j].reshape(64, 256).astype(F32))
            total = total + nxt[:, 128:] + dot(nxt[:, :128], total)
    h0 = h0 + dot(b2[:, :128], h0) + b2[:, 128:]
    h0 = h0 + dot(b1[:, :128], h0) + b1[:, 128:]

    for cp in staged[5:]:
        cp.wait()
    own_weight = jnp.concatenate([stw_ref[0:1], stw_ref[1:2]], 1)
    o = local_out[...]
    mech = dot(o[:, :128], h0) + o[:, 128:]
    ones = head_ones()
    rf, kf, vf = r_ref[...].astype(F32), k_ref[...].astype(F32), v_ref[...].astype(F32)
    centred = mech - dotx(mech, ones) * (1.0 / 64)
    spread = dotx(centred * centred, ones) * (1.0 / 64)
    token = dotx(rf * kf * own_weight, ones) * vf
    mixed = centred * lax.rsqrt(spread + GROUP_EPS) * hng_ref[...] + token
    mixed = (mixed / (1.0 + jnp.exp(-og_ref[...].astype(F32)))).astype(BF16)

    halves = (pl.ds(0, D // 2), pl.ds(D // 2, D // 2))
    Q = D // 4

    def sum_over_tp(n, a, columns_of, cb, meanwhile):
        other = 1 - core
        across = lax.rem(x + 2, NX)
        sides = (lax.rem(x + 1, NX), lax.rem(x + 3, NX))
        steps = (at(dx=1), at(dx=-1))

        def product(q):
            cut = pl.ds(q * Q, Q)
            prod = dot(a, columns_of(q * Q), 1, cb)
            for p in range(8):
                part[p // 2, p % 2, :, cut] = prod[p * ROWS : (p + 1) * ROWS].astype(BF16)
            push(
                part.at[:, other, :, cut], pair_in.at[n, :, :, cut], ps.at[n, q], pr.at[n, q],
                at(dc=1),
            )

        def add_pair(q):
            cut = pl.ds(q * Q, Q)
            landed(pair_in.at[n, :, :, cut], ps.at[n, q], pr.at[n, q])
            mine[n, :, :, cut] = (
                part[:, core, :, cut].astype(F32) + pair_in[n, :, :, cut].astype(F32)
            ).astype(BF16)

        def first_sends(e):
            push(
                mine.at[n, across, :, halves[e]], relay.at[n, e], xs.at[n, e], xr.at[n, e], steps[e]
            )
            push(
                mine.at[n, sides[1 - e], :, halves[e]], mix_in.at[n, 1 - e, :, halves[e]],
                xs.at[n, 3 - e], xr.at[n, 3 - e], steps[1 - e],
            )

        product(0)
        product(1)
        add_pair(0)
        product(2)
        add_pair(1)
        first_sends(0)
        product(3)
        meanwhile()
        add_pair(2)
        add_pair(3)
        first_sends(1)
        meanwhile()
        for e in range(2):
            landed(relay.at[n, e], xs.at[n, e], xr.at[n, e])
            joint[n, e] = (
                mine[n, sides[e], :, halves[e]].astype(F32) + relay[n, e].astype(F32)
            ).astype(BF16)
            push(
                joint.at[n, e], mix_in.at[n, e, :, halves[e]], xs.at[n, 4 + e], xr.at[n, 4 + e],
                steps[e],
            )
        meanwhile()
        total = mine[n, x].astype(F32)
        for e in range(2):
            landed(mix_in.at[n, e, :, halves[1 - e]], xs.at[n, 2 + e], xr.at[n, 2 + e])
            landed(mix_in.at[n, e, :, halves[e]], xs.at[n, 4 + e], xr.at[n, 4 + e])
            total = total + mix_in[n, e].astype(F32)
        return total

    def finish_sends():
        for cp in sends:
            cp.wait_send()
        sends.clear()

    service()
    mix = sum_over_tp(0, mixed, lambda c: wo_ref[:, c : c + Q], 0, service)
    mix = mix.astype(BF16).astype(F32)
    fetch.wait()
    after = (resid[...].astype(F32) + mix).astype(BF16).astype(F32)
    factor = lax.rsqrt(jnp.mean(after * after, axis=-1, keepdims=True) + NORM_EPS)
    normed = (after * factor * png_ref[...]).astype(BF16)

    rows_buf[x, core] = normed
    mine_rows = rows_buf.at[x, core]
    for e in range(2):
        b = rows_buf.at[x, core, :, halves[e]]
        push(b, b, gs.at[e, 0], gr.at[e, 0], at(dx=1 if e == 0 else -1))
    for e in range(2):
        b = rows_buf.at[x, core, :, halves[1 - e]]
        push(b, b, gs.at[e, 1], gr.at[e, 1], at(dx=1 if e == 0 else -1))
    push(mine_rows, mine_rows, fs.at[0], fr.at[0], at(dc=1))
    service()
    service()

    def came(dx, e, half, i, k, onward):
        b = rows_buf.at[lax.rem(x + dx, NX), core, :, halves[half]]
        landed(b, gs.at[e, i], gr.at[e, i])
        if onward:
            push(b, b, gs.at[e, 2], gr.at[e, 2], at(dx=1 if e == 0 else -1))
        push(b, b, fs.at[k], fr.at[k], at(dc=1))

    came(3, 0, 0, 0, 1, True)
    came(1, 1, 1, 0, 2, True)
    came(3, 0, 1, 1, 3, False)
    came(1, 1, 0, 1, 4, False)
    service()
    came(2, 0, 0, 2, 5, False)
    came(2, 1, 1, 2, 6, False)
    landed(rows_buf.at[x, 1 - core], fs.at[0], fr.at[0])
    for k, (dx, half) in enumerate(((3, 0), (1, 1), (3, 1), (1, 0), (2, 0), (2, 1))):
        b = rows_buf.at[lax.rem(x + dx, NX), 1 - core, :, halves[half]]
        landed(b, fs.at[k + 1], fr.at[k + 1])
    for j in range(8):
        nrm[j * ROWS : (j + 1) * ROWS] = rows_buf[j // 2, j % 2]

    gate = jnp.zeros((N, FF), F32)
    upper = jnp.zeros((N, FF), F32)
    arrivals = [o for t in range(9) for o in offsets(t)]
    for j in range(8):
        s_last = abs(arrivals[2 * j + 1])
        while turn[0] < min(3 * (s_last + 1) + 3, TURNS):
            one_turn()
        if turn[0] < TURNS:
            one_turn()
        two = arrivals[2 * j : 2 * j + 2]
        for o in two:
            y_end(o)
        cuts = [pl.ds(pl.multiple_of(lax.rem(z + o + NZ, NZ) * 128, 128), 128) for o in two]
        a = jnp.concatenate([nrm[:, cut] for cut in cuts], 1)
        wide = [gu[pl.ds(column(o), NY)] for o in two]
        gate = gate + dot(a, jnp.concatenate([w[:, :W].reshape(128, FF) for w in wide], 0))
        upper = upper + dot(a, jnp.concatenate([w[:, W:].reshape(128, FF) for w in wide], 0))
    assert turn[0] == TURNS
    hidden = (gate / (1.0 + jnp.exp(-gate)) * upper).astype(BF16)
    finish_sends()
    down = sum_over_tp(1, hidden, lambda c: dn[c // W : (c + Q) // W].reshape(Q, FF), 1, lambda: None)
    out_ref[...] = (after + down).astype(BF16)
    finish_sends()


def per_device(r, k, v, dec, lr, og, stw, hng, wo, res, png, wg, wu, wd):
    vmem = pl.BlockSpec(memory_space=pltpu.VMEM)
    hbm = pl.BlockSpec(memory_space=pl.ANY)
    dma = pltpu.SemaphoreType.DMA
    return pl.pallas_call(
        kernel,
        out_shape=jax.ShapeDtypeStruct((ROWS, D), BF16),
        in_specs=[hbm] * 14,
        out_specs=vmem,
        scratch_shapes=[
            *[pltpu.VMEM((N, 128), BF16)] * 3,
            *[pltpu.VMEM((N, 128), F32)] * 2,
            pltpu.VMEM((N, 128), BF16),
            pltpu.VMEM((2, 64), F32),
            pltpu.VMEM((1, 128), F32),
            pltpu.VMEM((128, D), BF16),
            pltpu.VMEM((1, D), F32),
            pltpu.VMEM((64, 2 * W, FF), BF16),
            pltpu.VMEM((64, W, FF), BF16),
            pltpu.VMEM((2, 4, 64, 256), BF16),
            pltpu.VMEM((4, NY, 16, 256), BF16),
            pltpu.VMEM((NX, NC, ROWS, D), BF16),
            pltpu.VMEM((2, NX, ROWS, D), BF16),
            pltpu.VMEM((2, NX, ROWS, D), BF16),
            pltpu.VMEM((2, 2, ROWS, D), BF16),
            pltpu.VMEM((2, 2, ROWS, D // 2), BF16),
            pltpu.VMEM((2, 2, ROWS, D // 2), BF16),
            pltpu.VMEM((NX, NC, ROWS, D), BF16),
            pltpu.VMEM((N, D), BF16),
            pltpu.VMEM((N, 256), F32),
            pltpu.VMEM((ROWS, D), BF16),
            dma((4,)), dma((10,)), pltpu.SemaphoreType.REGULAR((2, 7)),
            dma((2, 8)), dma((2, 8)),
            dma((16, 4)), dma((16, 4)),
            dma((3,)), dma((3,)),
            dma((2, 2, 8)), dma((2, 2, 8)),
            dma((4, 3)), dma((4, 3)),
            dma((2, 4)), dma((2, 4)),
            dma((2, 6)), dma((2, 6)),
            dma((2, 3)), dma((2, 3)),
            dma((7,)), dma((7,)),
        ],
        compiler_params=pltpu.CompilerParams(
            collective_id=0, has_side_effects=True, vmem_limit_bytes=60 * 1024 * 1024
        ),
        name="layer",
    )(r, k, v, dec, lr, og, stw, hng.reshape(1, 128), wo, res,
      png.reshape(1, D), wg, wu, wd.T)


def solution(mesh):
    torus = Mesh(mesh.devices.reshape(NZ, NY, NX, NC), ("z", "y", "x", "c"))
    sp, tp = ("z", "y"), ("x", "c")
    seq = P(sp, tp)
    return jax.shard_map(
        per_device,
        mesh=torus,
        in_specs=(
            seq, seq, seq, seq, seq, seq, P(tp, None), P(tp), P(tp, None), P(sp, None), P(),
            seq, seq, P(tp, sp),
        ),
        out_specs=P((*sp, *tp), None),
        check_vma=False,
    )
```

```python
import functools
import math

import jax
import jax.numpy as jnp
from jax import lax
from jax.experimental import pallas as pl
from jax.experimental.pallas import tpu as pltpu
from jax.sharding import Mesh
from jax.sharding import PartitionSpec as P

F32, BF16 = jnp.float32, jnp.bfloat16
MESH = pl.DeviceIdType.MESH
GROUP_EPS = 0.00064
NORM_EPS = 1e-06

NZ, NY, NX, NC = 16, 4, 4, 2
N = 192
ROWS = 24
D = 2048
FF = 640
W = 32
TURNS = 28
PLAN = (1, 2, 4, 4, 7, 8, 10, 11, 13, 14, 16, 17, 19, 20, 22, 23, 25, 26)


def dot(a, b, ca=1, cb=0):
    return lax.dot_general(
        a.astype(BF16), b.astype(BF16), (((ca,), (cb,)), ((), ())), preferred_element_type=F32
    )


def split(a):
    high = a.astype(BF16)
    return high, (a - high.astype(F32)).astype(BF16)


def dot3(a, b):
    (ah, al), (bh, bl) = split(a), split(b)
    return dot(ah, bh) + (dot(ah, bl) + dot(al, bh))


def head_sums(a):
    high, low = split(a)
    ones = head_ones().astype(BF16)
    return dot(jnp.concatenate([high, low], 1), jnp.concatenate([ones, ones], 0))


def running_sums(a):
    n = a.shape[0]
    high, low = split(a)
    tri = jnp.where(iota((n, n), 0) >= iota((n, n), 1), 1.0, 0.0).astype(BF16)
    sums = dot(tri, jnp.concatenate([high, low], 1))
    return sums[:, : a.shape[1]] + sums[:, a.shape[1] :]


def iota(shape, d):
    return lax.broadcasted_iota(jnp.int32, shape, d)


def head_ones():
    return jnp.where(iota((128, 128), 0) // 64 == iota((128, 128), 1) // 64, 1.0, 0.0).astype(F32)


def invert(low):
    n = low.shape[0]
    row, col = iota((n, n), 0), iota((n, n), 1)
    eye = jnp.where(row == col, 1.0, 0.0).astype(F32)
    d = jnp.where(row // 8 == col // 8, low, 0.0)
    d2 = dot3(d, d)
    d4 = dot3(d2, d2)
    x = eye + d
    x = x + dot3(d2, x)
    x = x + dot3(d4, x)
    m = 8
    while m < 64:
        off = jnp.where((row // (2 * m) == col // (2 * m)) & (row // m != col // m), low, 0.0)
        x = x + dot(x, dot(off, x))
        m *= 2
    off = jnp.where(row // 64 != col // 64, low, 0.0)
    y = dot(x, off)
    z = dot(y, x)
    return x + z + dot(y, z)


def local_scan(r, k, v, dec, lr, service):
    r, k, v = r.astype(F32), k.astype(F32), v.astype(F32)
    lw = (-math.exp(-0.5)) / (1.0 + jnp.exp(-dec))
    row, col = iota((N, N), 0), iota((N, N), 1)
    c = running_sums(lw)
    norm = jnp.sqrt(head_sums(k * k))
    unit = k / jnp.maximum(norm, 1.0)
    ins = unit / (1.0 + jnp.exp(-lr))
    up, dn = jnp.exp(c), jnp.exp(-c)
    last = c[N - 1 : N]
    rest = jnp.exp(last - c)
    at = -unit * jnp.exp(c - lw)
    rt = r * up
    left = jnp.concatenate([at, rt], 0)
    right = jnp.concatenate([ins * dn, k * dn], 0).astype(BF16)
    lane2 = iota((N, 256), 1) % 128
    us, reads = [], []
    for h in range(2):
        head_lanes = iota((2 * N, 128), 1) // 64 == h
        g = dot(jnp.where(head_lanes, left, 0.0), right, 1, 1)
        low = jnp.where(row > col, g[:N, :N], 0.0)
        mak = jnp.where(row > col, g[:N, N:], 0.0)
        mrb = jnp.where(row >= col, g[N:, :N], 0.0)
        mrk = jnp.where(row >= col, g[N:, N:], 0.0)
        x = invert(low)
        service()
        u = dot(x, jnp.concatenate([at, dot(mak, v)], 1))
        us.append(u)
        reads.append((mrb, mrk))
        if h == 1:
            service()
    u = jnp.where(lane2 < 64, us[0], us[1])
    f = dot((ins * rest).T, u)
    fl = f[:, 128:] + dot((k * rest).T, v)
    ones = head_ones()
    r1, c1 = iota((128, 128), 0), iota((128, 128), 1)
    e = f[:, :128] * ones + jnp.where(r1 == c1, jnp.exp(last) - 1.0, 0.0)
    l = fl * ones

    def outputs():
        outs = []
        for h in range(2):
            mrb, mrk = reads[h]
            o = dot(mrb, us[h])
            ov = dot(mrk, v)
            outs.append(jnp.concatenate([o[:, :128] + rt, o[:, 128:] + ov], 1))
        return jnp.where(lane2 < 64, outs[0], outs[1])

    return e[:64] + e[64:], l[:64] + l[64:], outputs


def after_of(first, then):
    return first + then + dot(then[:, :128], first)


def unpack(p):
    first = iota(p.shape, 1) % 128 < 64
    return jnp.concatenate([jnp.where(first, p, 0.0), jnp.where(first, 0.0, p)], 0)


def pack(p):
    first = iota((64, p.shape[1]), 1) % 128 < 64
    return jnp.where(first, p[:64], p[64:])


def kernel(
    r_in, k_in, v_in, dec_in, lr_in, og_in, stw_in, hng_in, wo_in, res_ref, png_in,
    wg_ref, wu_ref, wd_ref,
    out_ref,
    r_ref, k_ref, v_ref, dec_ref, lr_ref, og_ref, stw_ref, hng_ref, wo_ref, png_ref,
    gu, dn, state, far, part, pair_in, mine, mix_in, rows_buf, nrm, local_out, resid,
    loc_sem, in_sem, word, zs, zr, ys, yr, as_, ar, azs, azr, ss, sr, ps, pr, xs, xr, gs, gr, fs, fr,
):
    z, y, x, core = (lax.axis_index(a) for a in ("z", "y", "x", "c"))
    here = z * NY + y

    def at(dz=0, dy=0, dx=0, dc=0):
        return (
            lax.rem(z + dz + NZ, NZ), lax.rem(y + dy + NY, NY),
            lax.rem(x + dx + NX, NX), lax.rem(core + dc, NC),
        )

    sends, pair_sends = [], []

    def push(src, dst, send, recv, to):
        cp = pltpu.make_async_remote_copy(
            src_ref=src, dst_ref=dst, send_sem=send, recv_sem=recv, device_id=to,
            device_id_type=MESH,
        )
        cp.start()
        sends.append(cp)
        return cp

    def landed(dst, send, recv):
        pltpu.make_async_remote_copy(
            src_ref=dst, dst_ref=dst, send_sem=send, recv_sem=recv, device_id=at(dz=1),
            device_id_type=MESH,
        ).wait_recv()

    own = [
        pltpu.make_async_copy(wg_ref, gu.at[here, pl.ds(0, W)], loc_sem.at[0]),
        pltpu.make_async_copy(wu_ref, gu.at[here, pl.ds(W, W)], loc_sem.at[1]),
        pltpu.make_async_copy(wd_ref, dn.at[here], loc_sem.at[2]),
    ]
    row0 = pl.multiple_of((x * NC + core) * ROWS, 8)
    fetch = pltpu.make_async_copy(res_ref.at[pl.ds(row0, ROWS)], resid, loc_sem.at[3])

    zb, za = z % 4, z // 4
    peers = [at(dz=1), at(dz=-1), at(dy=1), at(dy=2), at(dy=3)]
    peers += [at(dx=1), at(dx=2), at(dx=3), at(dc=1)]
    z_near = [(za * 4 + lax.rem(zb + d, 4), y, x, core) for d in (1, 2, 3)]
    z_far = [at(dz=4 * d) for d in (1, 2, 3)]
    barrier = pltpu.get_barrier_semaphore()
    for p in peers:
        pl.semaphore_signal(barrier, inc=1, device_id=p, device_id_type=MESH)
    pairs = (
        (r_in, r_ref), (k_in, k_ref), (v_in, v_ref), (dec_in, dec_ref), (lr_in, lr_ref),
        (og_in, og_ref), (stw_in, stw_ref), (hng_in, hng_ref), (wo_in, wo_ref), (png_in, png_ref),
    )
    staged = [pltpu.make_async_copy(a, b, in_sem.at[i]) for i, (a, b) in enumerate(pairs)]
    for cp in (*own, *staged, fetch):
        cp.start()
    for cp in own:
        cp.wait()
    pl.semaphore_wait(barrier, len(peers))

    def word_on(t):
        for d in range(2):
            to = at(dz=2**t if d == 0 else -(2**t))
            pl.semaphore_signal(word.at[d, t], inc=1, device_id=to, device_id_type=MESH)

    def word_in(t):
        for d in range(2):
            pl.semaphore_wait(word.at[d, t], 1)

    word_on(0)

    def slot(dz, dy=0):
        return lax.rem(z + dz + NZ, NZ) * NY + lax.rem(y + dy + NY, NY)

    def column(dz):
        return pl.multiple_of(lax.rem(z + dz + NZ, NZ) * NY, NY)

    def offsets(s):
        return [0] if s == 0 else ([-s, s] if s < 8 else [8])

    def index(o):
        return 0 if o == 0 else (15 if o == 8 else 2 * abs(o) - (1 if o < 0 else 0))

    def y_out(o):
        i = index(o)
        src = gu.at[slot(o)]
        push(src, src, ys.at[i, 0], yr.at[i, 0], at(dy=1))
        push(src, src, ys.at[i, 1], yr.at[i, 1], at(dy=-1))

    def y_on(o):
        i = index(o)
        a, b = gu.at[slot(o, -1)], gu.at[slot(o, 1)]
        landed(a, ys.at[i, 0], yr.at[i, 0])
        a = gu.at[slot(o, -1), pl.ds(0, W)]
        push(a, a, ys.at[i, 2], yr.at[i, 2], at(dy=1))
        landed(b, ys.at[i, 1], yr.at[i, 1])
        b = gu.at[slot(o, 1), pl.ds(W, W)]
        push(b, b, ys.at[i, 3], yr.at[i, 3], at(dy=-1))

    def y_end(o):
        i = index(o)
        landed(gu.at[slot(o, 2), pl.ds(0, W)], ys.at[i, 2], yr.at[i, 2])
        landed(gu.at[slot(o, 2), pl.ds(W, W)], ys.at[i, 3], yr.at[i, 3])

    def z_block(dz, d, s):
        b = gu.at[slot(dz)]
        return b if s < 8 else gu.at[slot(dz), pl.ds(W * d, W)]

    def z_out(s):
        for d in range(2):
            o = -s if d == 0 else s
            b = z_block(o, d, s + 1)
            push(b, b, zs.at[d, s], zr.at[d, s], at(dz=1 if d == 0 else -1))

    def z_in(s):
        for d in range(2):
            landed(z_block(-s if d == 0 else s, d, s), zs.at[d, s - 1], zr.at[d, s - 1])

    def a_dirs(s, g):
        return (0, 1) if s < 8 else (g,)

    def a_block(s, d, g):
        return dn.at[pl.ds(column(-s if d == 0 else s) + 2 * g, 2)]

    def a_out(s, g):
        for d in a_dirs(s + 1, g):
            b = a_block(s, d, g)
            push(b, b, azs.at[d, g, s], azr.at[d, g, s], at(dz=1 if d == 0 else -1))

    def a_in(s, g):
        for d in a_dirs(s, g):
            landed(a_block(s, d, g), azs.at[d, g, s - 1], azr.at[d, g, s - 1])

    turn, points = [0], [0]

    def service():
        points[0] += 1
        while turn[0] < PLAN[points[0] - 1]:
            one_turn()

    def one_turn():
        s, g = divmod(turn[0], 3)
        turn[0] += 1
        if turn[0] in (2, 4):
            word_in(turn[0] // 2 - 1)
            word_on(turn[0] // 2)
        if turn[0] == 7:
            word_in(2)
        if s == 0 and g == 0:
            z_out(0)
            for d in (1, 3, 2):
                push(dn.at[here], dn.at[here], as_.at[d - 1], ar.at[d - 1], at(dy=d))
            y_out(0)
        elif s <= 8 and g == 0:
            z_in(s)
            if s < 8:
                z_out(s)
            for o in offsets(s):
                y_out(o)
        elif s <= 8:
            if s == 0 and g == 1:
                for d in (1, 2, 3):
                    landed(dn.at[slot(0, -d)], as_.at[d - 1], ar.at[d - 1])
            if s > 0:
                a_in(s, g - 1)
            if s < 8:
                a_out(s, g - 1)
            if s > 0:
                for o in offsets(s - 1)[g - 1 : g]:
                    y_on(o)
        else:
            for o in offsets(8):
                y_on(o)

    service()

    for cp in staged[:5]:
        cp.wait()

    e, l, outputs = local_scan(
        r_ref[...], k_ref[...], v_ref[...], dec_ref[...], lr_ref[...], service
    )

    def level(n, x_own, mates, place, meanwhile):
        state[n, place, :, :128] = x_own[0].astype(BF16)
        state[n, place, :, 128:] = x_own[1].astype(BF16)
        for d in (2, 1, 3):
            b = state.at[n, place]
            push(b, b, ss.at[n, d - 1], sr.at[n, d - 1], mates[d - 1])
        meanwhile()
        for d in (1, 3, 2):
            landed(state.at[n, lax.rem(place - d + 4, 4)], ss.at[n, d - 1], sr.at[n, d - 1])
        m = [unpack(state[n, j].astype(F32)) for j in range(4)]
        m01, m23 = after_of(m[0], m[1]), after_of(m[2], m[3])
        m012, total = after_of(m01, m[2]), after_of(m01, m23)
        before = jnp.where(place == 1, m[0], jnp.zeros_like(total))
        before = jnp.where(place == 2, m01, jnp.where(place == 3, m012, before))
        return total, before

    def meanwhile_outputs():
        service()
        local_out[...] = outputs()
        service()

    def meanwhile_services():
        service()
        service()

    y_mates = [at(dy=d) for d in (1, 2, 3)]
    t1, b1 = level(0, (e, l), y_mates, y, meanwhile_outputs)
    p1 = pack(t1)
    t2, b2 = level(1, (p1[:, :128], p1[:, 128:]), z_near, zb, meanwhile_services)

    p2 = pack(t2).astype(BF16)
    quarter = jnp.zeros((16, 256), BF16)
    for j in range(4):
        quarter = jnp.where(y == j, p2[j * 16 : (j + 1) * 16], quarter)
    far[za, y] = quarter
    for d in (2, 1, 3):
        b = far.at[za, y]
        push(b, b, ss.at[2, d - 1], sr.at[2, d - 1], z_far[d - 1])
    service()
    service()
    for d in (1, 3, 2):
        landed(far.at[lax.rem(za - d + 4, 4), y], ss.at[2, d - 1], sr.at[2, d - 1])
    for d in (2, 1, 3):
        b = far.at[:, y]
        push(b, b, ss.at[3, d - 1], sr.at[3, d - 1], y_mates[d - 1])
    service()
    for d in (1, 3, 2):
        landed(far.at[:, lax.rem(y - d + 4, 4)], ss.at[3, d - 1], sr.at[3, d - 1])
    total = unpack(far[0].reshape(64, 256)[:, 128:].astype(F32))
    h0 = jnp.zeros_like(total)
    for j in range(1, 4):
        h0 = jnp.where(za == j, total, h0)
        if j < 3:
            nxt = unpack(far[j].reshape(64, 256).astype(F32))
            total = total + nxt[:, 128:] + dot(nxt[:, :128], total)
    h0 = h0 + dot(b2[:, :128], h0) + b2[:, 128:]
    h0 = h0 + dot(b1[:, :128], h0) + b1[:, 128:]

    for cp in staged[5:]:
        cp.wait()
    own_weight = jnp.concatenate([stw_ref[0:1], stw_ref[1:2]], 1)
    o = local_out[...]
    mech = dot(o[:, :128], h0) + o[:, 128:]
    rf, kf, vf = r_ref[...].astype(F32), k_ref[...].astype(F32), v_ref[...].astype(F32)
    centred = mech - head_sums(mech) * (1.0 / 64)
    spread = head_sums(centred * centred) * (1.0 / 64)
    token = head_sums(rf * kf * own_weight) * vf
    mixed = centred * lax.rsqrt(spread + GROUP_EPS) * hng_ref[...] + token
    mixed = (mixed / (1.0 + jnp.exp(-og_ref[...].astype(F32)))).astype(BF16)

    halves = (pl.ds(0, D // 2), pl.ds(D // 2, D // 2))
    Q = D // 4

    def sum_over_tp(n, a, columns_of, cb, meanwhile):
        other = 1 - core

        def product(q):
            cut = pl.ds(q * Q, Q)
            prod = dot(a, columns_of(q * Q), 1, cb)
            for p in range(8):
                part[p // 2, p % 2, :, cut] = prod[p * ROWS : (p + 1) * ROWS].astype(BF16)
            cp = push(
                part.at[:, other, :, cut], pair_in.at[n, :, :, cut], ps.at[n, q], pr.at[n, q],
                at(dc=1),
            )
            if n == 0:
                pair_sends.append(cp)

        def add_pair(q):
            cut = pl.ds(q * Q, Q)
            landed(pair_in.at[n, :, :, cut], ps.at[n, q], pr.at[n, q])
            mine[n, :, :, cut] = (
                part[:, core, :, cut].astype(F32) + pair_in[n, :, :, cut].astype(F32)
            ).astype(BF16)

        def first_sends(e):
            for d in (2, 1, 3):
                push(
                    mine.at[n, lax.rem(x + d, NX), :, halves[e]], mix_in.at[n, d - 1, :, halves[e]],
                    xs.at[n, e, d - 1], xr.at[n, e, d - 1], at(dx=d),
                )

        product(0)
        product(1)
        add_pair(0)
        product(2)
        add_pair(1)
        first_sends(0)
        product(3)
        meanwhile()
        add_pair(2)
        add_pair(3)
        first_sends(1)
        meanwhile()
        meanwhile()
        total = mine[n, x].astype(F32)
        for d in (1, 3, 2):
            for e in range(2):
                landed(mix_in.at[n, d - 1, :, halves[e]], xs.at[n, e, d - 1], xr.at[n, e, d - 1])
            total = total + mix_in[n, d - 1].astype(F32)
        return total

    def finish_sends():
        for cp in sends:
            cp.wait_send()
        sends.clear()

    service()
    mix = sum_over_tp(0, mixed, lambda c: wo_ref[:, c : c + Q], 0, service)
    mix = mix.astype(BF16).astype(F32)
    fetch.wait()
    after = (resid[...].astype(F32) + mix).astype(BF16).astype(F32)
    factor = lax.rsqrt(jnp.mean(after * after, axis=-1, keepdims=True) + NORM_EPS)
    normed = (after * factor * png_ref[...]).astype(BF16)

    rows_buf[x, core] = normed
    mine_rows = rows_buf.at[x, core]
    for d in (2, 1, 3):
        push(mine_rows, mine_rows, gs.at[d - 1], gr.at[d - 1], at(dx=d))
    push(mine_rows, mine_rows, fs.at[0], fr.at[0], at(dc=1))
    service()
    service()
    for d in (1, 3, 2):
        b = rows_buf.at[lax.rem(x + NX - d, NX), core]
        landed(b, gs.at[d - 1], gr.at[d - 1])
        push(b, b, fs.at[d], fr.at[d], at(dc=1))
    service()
    for d in (0, 1, 3, 2):
        landed(rows_buf.at[lax.rem(x + NX - d, NX), 1 - core], fs.at[d], fr.at[d])
    for j in range(8):
        nrm[j * ROWS : (j + 1) * ROWS] = rows_buf[j // 2, j % 2]

    gate = jnp.zeros((N, FF), F32)
    upper = jnp.zeros((N, FF), F32)
    arrivals = [o for t in range(9) for o in offsets(t)]
    for j in range(8):
        s_last = abs(arrivals[2 * j + 1])
        while turn[0] < min(3 * (s_last + 1) + 3, TURNS):
            one_turn()
        if turn[0] < TURNS:
            one_turn()
        two = arrivals[2 * j : 2 * j + 2]
        for o in two:
            y_end(o)
        cuts = [pl.ds(pl.multiple_of(lax.rem(z + o + NZ, NZ) * 128, 128), 128) for o in two]
        a = jnp.concatenate([nrm[:, cut] for cut in cuts], 1)
        wide = [gu[pl.ds(column(o), NY)] for o in two]
        gate = gate + dot(a, jnp.concatenate([w[:, :W].reshape(128, FF) for w in wide], 0))
        upper = upper + dot(a, jnp.concatenate([w[:, W:].reshape(128, FF) for w in wide], 0))
    assert turn[0] == TURNS
    hidden = (gate / (1.0 + jnp.exp(-gate)) * upper).astype(BF16)
    for cp in pair_sends:
        cp.wait_send()
    sends[:] = [cp for cp in sends if all(cp is not p for p in pair_sends)]
    down = sum_over_tp(1, hidden, lambda c: dn[c // W : (c + Q) // W].reshape(Q, FF), 1, lambda: None)
    out_ref[...] = (after + down).astype(BF16)
    finish_sends()


def per_device(r, k, v, dec, lr, og, stw, hng, wo, res, png, wg, wu, wd):
    vmem = pl.BlockSpec(memory_space=pltpu.VMEM)
    hbm = pl.BlockSpec(memory_space=pl.ANY)
    dma = pltpu.SemaphoreType.DMA
    return pl.pallas_call(
        kernel,
        out_shape=jax.ShapeDtypeStruct((ROWS, D), BF16),
        in_specs=[hbm] * 14,
        out_specs=vmem,
        scratch_shapes=[
            *[pltpu.VMEM((N, 128), BF16)] * 3,
            *[pltpu.VMEM((N, 128), F32)] * 2,
            pltpu.VMEM((N, 128), BF16),
            pltpu.VMEM((2, 64), F32),
            pltpu.VMEM((1, 128), F32),
            pltpu.VMEM((128, D), BF16),
            pltpu.VMEM((1, D), F32),
            pltpu.VMEM((64, 2 * W, FF), BF16),
            pltpu.VMEM((64, W, FF), BF16),
            pltpu.VMEM((2, 4, 64, 256), BF16),
            pltpu.VMEM((4, NY, 16, 256), BF16),
            pltpu.VMEM((NX, NC, ROWS, D), BF16),
            pltpu.VMEM((2, NX, ROWS, D), BF16),
            pltpu.VMEM((2, NX, ROWS, D), BF16),
            pltpu.VMEM((2, 3, ROWS, D), BF16),
            pltpu.VMEM((NX, NC, ROWS, D), BF16),
            pltpu.VMEM((N, D), BF16),
            pltpu.VMEM((N, 256), F32),
            pltpu.VMEM((ROWS, D), BF16),
            dma((4,)), dma((10,)), pltpu.SemaphoreType.REGULAR((2, 3)),
            dma((2, 8)), dma((2, 8)),
            dma((16, 4)), dma((16, 4)),
            dma((3,)), dma((3,)),
            dma((2, 2, 8)), dma((2, 2, 8)),
            dma((4, 3)), dma((4, 3)),
            dma((2, 4)), dma((2, 4)),
            dma((2, 2, 3)), dma((2, 2, 3)),
            dma((3,)), dma((3,)),
            dma((4,)), dma((4,)),
        ],
        compiler_params=pltpu.CompilerParams(
            collective_id=0, has_side_effects=True, vmem_limit_bytes=60 * 1024 * 1024
        ),
        name="layer",
    )(r, k, v, dec, lr, og, stw, hng.reshape(1, 128), wo, res,
      png.reshape(1, D), wg, wu, wd.T)


def solution(mesh):
    torus = Mesh(mesh.devices.reshape(NZ, NY, NX, NC), ("z", "y", "x", "c"))
    sp, tp = ("z", "y"), ("x", "c")
    seq = P(sp, tp)
    return jax.shard_map(
        per_device,
        mesh=torus,
        in_specs=(
            seq, seq, seq, seq, seq, seq, P(tp, None), P(tp), P(tp, None), P(sp, None), P(),
            seq, seq, P(tp, sp),
        ),
        out_specs=P((*sp, *tp), None),
        check_vma=False,
    )
```

```python
import functools
import math

import jax
import jax.numpy as jnp
from jax import lax
from jax.experimental import pallas as pl
from jax.experimental.pallas import tpu as pltpu
from jax.sharding import Mesh
from jax.sharding import PartitionSpec as P

F32, BF16 = jnp.float32, jnp.bfloat16
MESH = pl.DeviceIdType.MESH
GROUP_EPS = 0.00064
NORM_EPS = 1e-06

NZ, NY, NX, NC = 16, 4, 4, 2
N = 192
ROWS = 24
D = 2048
FF = 640
W = 32
TURNS = 28
PLAN = (1, 2, 4, 4, 7, 8, 10, 11, 13, 14, 16, 17, 19, 20, 22, 23, 25, 26)


def dot(a, b, ca=1, cb=0):
    return lax.dot_general(
        a.astype(BF16), b.astype(BF16), (((ca,), (cb,)), ((), ())), preferred_element_type=F32
    )


def split(a):
    high = a.astype(BF16)
    return high, (a - high.astype(F32)).astype(BF16)


def dot3(a, b):
    (ah, al), (bh, bl) = split(a), split(b)
    return dot(ah, bh) + (dot(ah, bl) + dot(al, bh))


def head_sums(a):
    high, low = split(a)
    ones = head_ones().astype(BF16)
    return dot(jnp.concatenate([high, low], 1), jnp.concatenate([ones, ones], 0))


def running_sums(a):
    n = a.shape[0]
    high, low = split(a)
    tri = jnp.where(iota((n, n), 0) >= iota((n, n), 1), 1.0, 0.0).astype(BF16)
    sums = dot(tri, jnp.concatenate([high, low], 1))
    return sums[:, : a.shape[1]] + sums[:, a.shape[1] :]


def iota(shape, d):
    return lax.broadcasted_iota(jnp.int32, shape, d)


def head_ones():
    return jnp.where(iota((128, 128), 0) // 64 == iota((128, 128), 1) // 64, 1.0, 0.0).astype(F32)


def invert(low):
    n = low.shape[0]
    row, col = iota((n, n), 0), iota((n, n), 1)
    eye = jnp.where(row == col, 1.0, 0.0).astype(F32)
    d = jnp.where(row // 8 == col // 8, low, 0.0)
    d2 = dot3(d, d)
    d4 = dot3(d2, d2)
    x = eye + d
    x = x + dot3(d2, x)
    x = x + dot3(d4, x)
    m = 8
    while m < 64:
        off = jnp.where((row // (2 * m) == col // (2 * m)) & (row // m != col // m), low, 0.0)
        x = x + dot(x, dot(off, x))
        m *= 2
    off = jnp.where(row // 64 != col // 64, low, 0.0)
    y = dot(x, off)
    z = dot(y, x)
    return x + z + dot(y, z)


def local_scan(r, k, v, dec, lr, service):
    r, k, v = r.astype(F32), k.astype(F32), v.astype(F32)
    lw = (-math.exp(-0.5)) / (1.0 + jnp.exp(-dec))
    row, col = iota((N, N), 0), iota((N, N), 1)
    c = running_sums(lw)
    norm = jnp.sqrt(head_sums(k * k))
    unit = k / jnp.maximum(norm, 1.0)
    ins = unit / (1.0 + jnp.exp(-lr))
    up, dn = jnp.exp(c), jnp.exp(-c)
    last = c[N - 1 : N]
    rest = jnp.exp(last - c)
    at = -unit * jnp.exp(c - lw)
    rt = r * up
    left = jnp.concatenate([at, rt], 0)
    right = jnp.concatenate([ins * dn, k * dn], 0).astype(BF16)
    lane2 = iota((N, 256), 1) % 128
    us, reads = [], []
    for h in range(2):
        head_lanes = iota((2 * N, 128), 1) // 64 == h
        g = dot(jnp.where(head_lanes, left, 0.0), right, 1, 1)
        low = jnp.where(row > col, g[:N, :N], 0.0)
        mak = jnp.where(row > col, g[:N, N:], 0.0)
        mrb = jnp.where(row >= col, g[N:, :N], 0.0)
        mrk = jnp.where(row >= col, g[N:, N:], 0.0)
        x = invert(low)
        service()
        u = dot(x, jnp.concatenate([at, dot(mak, v)], 1))
        us.append(u)
        reads.append((mrb, mrk))
        if h == 1:
            service()
    u = jnp.where(lane2 < 64, us[0], us[1])
    f = dot((ins * rest).T, u)
    fl = f[:, 128:] + dot((k * rest).T, v)
    ones = head_ones()
    r1, c1 = iota((128, 128), 0), iota((128, 128), 1)
    e = f[:, :128] * ones + jnp.where(r1 == c1, jnp.exp(last) - 1.0, 0.0)
    l = fl * ones

    def outputs():
        outs = []
        for h in range(2):
            mrb, mrk = reads[h]
            o = dot(mrb, us[h])
            ov = dot(mrk, v)
            outs.append(jnp.concatenate([o[:, :128] + rt, o[:, 128:] + ov], 1))
        return jnp.where(lane2 < 64, outs[0], outs[1])

    return e[:64] + e[64:], l[:64] + l[64:], outputs


def after_of(first, then):
    return first + then + dot(then[:, :128], first)


def unpack(p):
    first = iota(p.shape, 1) % 128 < 64
    return jnp.concatenate([jnp.where(first, p, 0.0), jnp.where(first, 0.0, p)], 0)


def pack(p):
    first = iota((64, p.shape[1]), 1) % 128 < 64
    return jnp.where(first, p[:64], p[64:])


def kernel(
    r_in, k_in, v_in, dec_in, lr_in, og_in, stw_in, hng_in, wo_in, res_ref, png_in,
    wg_ref, wu_ref, wd_ref,
    out_ref,
    r_ref, k_ref, v_ref, dec_ref, lr_ref, og_ref, stw_ref, hng_ref, wo_ref, png_ref,
    gu, dn, state, far, part, pair_in, mine, mix_in, rows_buf, nrm, local_out, resid,
    loc_sem, in_sem, word, zs, zr, ys, yr, as_, ar, azs, azr, ss, sr, ps, pr, xs, xr, gs, gr, fs, fr,
):
    z, y, x, core = (lax.axis_index(a) for a in ("z", "y", "x", "c"))
    here = z * NY + y

    def at(dz=0, dy=0, dx=0, dc=0):
        return (
            lax.rem(z + dz + NZ, NZ), lax.rem(y + dy + NY, NY),
            lax.rem(x + dx + NX, NX), lax.rem(core + dc, NC),
        )

    sends, pair_sends = [], []

    def push(src, dst, send, recv, to):
        cp = pltpu.make_async_remote_copy(
            src_ref=src, dst_ref=dst, send_sem=send, recv_sem=recv, device_id=to,
            device_id_type=MESH,
        )
        cp.start()
        sends.append(cp)
        return cp

    def landed(dst, send, recv):
        pltpu.make_async_remote_copy(
            src_ref=dst, dst_ref=dst, send_sem=send, recv_sem=recv, device_id=at(dz=1),
            device_id_type=MESH,
        ).wait_recv()

    own = [
        pltpu.make_async_copy(wg_ref, gu.at[here, pl.ds(0, W)], loc_sem.at[0]),
        pltpu.make_async_copy(wu_ref, gu.at[here, pl.ds(W, W)], loc_sem.at[1]),
        pltpu.make_async_copy(wd_ref, dn.at[here], loc_sem.at[2]),
    ]
    row0 = pl.multiple_of((x * NC + core) * ROWS, 8)
    fetch = pltpu.make_async_copy(res_ref.at[pl.ds(row0, ROWS)], resid, loc_sem.at[3])

    zb, za = z % 4, z // 4
    peers = [at(dz=1), at(dz=-1), at(dy=1), at(dy=2), at(dy=3)]
    peers += [at(dx=1), at(dx=2), at(dx=3), at(dc=1)]
    z_near = [(za * 4 + lax.rem(zb + d, 4), y, x, core) for d in (1, 2, 3)]
    z_far = [at(dz=4 * d) for d in (1, 2, 3)]
    barrier = pltpu.get_barrier_semaphore()
    for p in peers:
        pl.semaphore_signal(barrier, inc=1, device_id=p, device_id_type=MESH)
    pairs = (
        (r_in, r_ref), (k_in, k_ref), (v_in, v_ref), (dec_in, dec_ref), (lr_in, lr_ref),
        (og_in, og_ref), (stw_in, stw_ref), (hng_in, hng_ref), (wo_in, wo_ref), (png_in, png_ref),
    )
    staged = [pltpu.make_async_copy(a, b, in_sem.at[i]) for i, (a, b) in enumerate(pairs)]
    for cp in (*own, *staged, fetch):
        cp.start()
    for cp in own:
        cp.wait()
    pl.semaphore_wait(barrier, len(peers))

    def word_on(t):
        for d in range(2):
            to = at(dz=2**t if d == 0 else -(2**t))
            pl.semaphore_signal(word.at[d, t], inc=1, device_id=to, device_id_type=MESH)

    def word_in(t):
        for d in range(2):
            pl.semaphore_wait(word.at[d, t], 1)

    word_on(0)

    def slot(dz, dy=0):
        return lax.rem(z + dz + NZ, NZ) * NY + lax.rem(y + dy + NY, NY)

    def column(dz):
        return pl.multiple_of(lax.rem(z + dz + NZ, NZ) * NY, NY)

    def offsets(s):
        return [0] if s == 0 else ([-s, s] if s < 8 else [8])

    def index(o):
        return 0 if o == 0 else (15 if o == 8 else 2 * abs(o) - (1 if o < 0 else 0))

    def y_out(o):
        i = index(o)
        src = gu.at[slot(o)]
        push(src, src, ys.at[i, 0], yr.at[i, 0], at(dy=1))
        push(src, src, ys.at[i, 1], yr.at[i, 1], at(dy=-1))

    def y_on(o):
        i = index(o)
        a, b = gu.at[slot(o, -1)], gu.at[slot(o, 1)]
        landed(a, ys.at[i, 0], yr.at[i, 0])
        a = gu.at[slot(o, -1), pl.ds(0, W)]
        push(a, a, ys.at[i, 2], yr.at[i, 2], at(dy=1))
        landed(b, ys.at[i, 1], yr.at[i, 1])
        b = gu.at[slot(o, 1), pl.ds(W, W)]
        push(b, b, ys.at[i, 3], yr.at[i, 3], at(dy=-1))

    def y_end(o):
        i = index(o)
        landed(gu.at[slot(o, 2), pl.ds(0, W)], ys.at[i, 2], yr.at[i, 2])
        landed(gu.at[slot(o, 2), pl.ds(W, W)], ys.at[i, 3], yr.at[i, 3])

    def z_block(dz, d, s):
        b = gu.at[slot(dz)]
        return b if s < 8 else gu.at[slot(dz), pl.ds(W * d, W)]

    def z_out(s):
        for d in range(2):
            o = -s if d == 0 else s
            b = z_block(o, d, s + 1)
            push(b, b, zs.at[d, s], zr.at[d, s], at(dz=1 if d == 0 else -1))

    def z_in(s):
        for d in range(2):
            landed(z_block(-s if d == 0 else s, d, s), zs.at[d, s - 1], zr.at[d, s - 1])

    def a_dirs(s, g):
        return (0, 1) if s < 8 else (g,)

    def a_block(s, d, g):
        return dn.at[pl.ds(column(-s if d == 0 else s) + 2 * g, 2)]

    def a_out(s, g):
        for d in a_dirs(s + 1, g):
            b = a_block(s, d, g)
            push(b, b, azs.at[d, g, s], azr.at[d, g, s], at(dz=1 if d == 0 else -1))

    def a_in(s, g):
        for d in a_dirs(s, g):
            landed(a_block(s, d, g), azs.at[d, g, s - 1], azr.at[d, g, s - 1])

    turn, points = [0], [0]

    def service():
        points[0] += 1
        while turn[0] < PLAN[points[0] - 1]:
            one_turn()

    def one_turn():
        s, g = divmod(turn[0], 3)
        turn[0] += 1
        if turn[0] in (2, 4):
            word_in(turn[0] // 2 - 1)
            word_on(turn[0] // 2)
        if turn[0] == 7:
            word_in(2)
        if s == 0 and g == 0:
            z_out(0)
            for d in (1, 3, 2):
                push(dn.at[here], dn.at[here], as_.at[d - 1], ar.at[d - 1], at(dy=d))
            y_out(0)
        elif s <= 8 and g == 0:
            z_in(s)
            if s < 8:
                z_out(s)
            for o in offsets(s):
                y_out(o)
        elif s <= 8:
            if s > 0:
                for o in offsets(s - 1)[g - 1 : g]:
                    y_on(o)
            if s == 0 and g == 1:
                for d in (1, 2, 3):
                    landed(dn.at[slot(0, -d)], as_.at[d - 1], ar.at[d - 1])
            if s > 0:
                a_in(s, g - 1)
            if s < 8:
                a_out(s, g - 1)
        else:
            for o in offsets(8):
                y_on(o)

    service()

    for cp in staged[:5]:
        cp.wait()

    e, l, outputs = local_scan(
        r_ref[...], k_ref[...], v_ref[...], dec_ref[...], lr_ref[...], service
    )

    def level(n, x_own, mates, place, meanwhile):
        state[n, place, :, :128] = x_own[0].astype(BF16)
        state[n, place, :, 128:] = x_own[1].astype(BF16)
        for d in (2, 1, 3):
            b = state.at[n, place]
            push(b, b, ss.at[n, d - 1], sr.at[n, d - 1], mates[d - 1])
        meanwhile()
        for d in (1, 3, 2):
            landed(state.at[n, lax.rem(place - d + 4, 4)], ss.at[n, d - 1], sr.at[n, d - 1])
        m = [unpack(state[n, j].astype(F32)) for j in range(4)]
        m01, m23 = after_of(m[0], m[1]), after_of(m[2], m[3])
        m012, total = after_of(m01, m[2]), after_of(m01, m23)
        before = jnp.where(place == 1, m[0], jnp.zeros_like(total))
        before = jnp.where(place == 2, m01, jnp.where(place == 3, m012, before))
        return total, before

    def meanwhile_outputs():
        service()
        local_out[...] = outputs()
        service()

    def meanwhile_services():
        service()
        service()

    y_mates = [at(dy=d) for d in (1, 2, 3)]
    t1, b1 = level(0, (e, l), y_mates, y, meanwhile_outputs)
    p1 = pack(t1)
    t2, b2 = level(1, (p1[:, :128], p1[:, 128:]), z_near, zb, meanwhile_services)

    p2 = pack(t2).astype(BF16)
    quarter = jnp.zeros((16, 256), BF16)
    for j in range(4):
        quarter = jnp.where(y == j, p2[j * 16 : (j + 1) * 16], quarter)
    far[za, y] = quarter
    for d in (2, 1, 3):
        b = far.at[za, y]
        push(b, b, ss.at[2, d - 1], sr.at[2, d - 1], z_far[d - 1])
    service()
    service()
    for d in (1, 3, 2):
        landed(far.at[lax.rem(za - d + 4, 4), y], ss.at[2, d - 1], sr.at[2, d - 1])
    for d in (2, 1, 3):
        b = far.at[:, y]
        push(b, b, ss.at[3, d - 1], sr.at[3, d - 1], y_mates[d - 1])
    service()
    for d in (1, 3, 2):
        landed(far.at[:, lax.rem(y - d + 4, 4)], ss.at[3, d - 1], sr.at[3, d - 1])
    total = unpack(far[0].reshape(64, 256)[:, 128:].astype(F32))
    h0 = jnp.zeros_like(total)
    for j in range(1, 4):
        h0 = jnp.where(za == j, total, h0)
        if j < 3:
            nxt = unpack(far[j].reshape(64, 256).astype(F32))
            total = total + nxt[:, 128:] + dot(nxt[:, :128], total)
    h0 = h0 + dot(b2[:, :128], h0) + b2[:, 128:]
    h0 = h0 + dot(b1[:, :128], h0) + b1[:, 128:]

    for cp in staged[5:]:
        cp.wait()
    own_weight = jnp.concatenate([stw_ref[0:1], stw_ref[1:2]], 1)
    o = local_out[...]
    mech = dot(o[:, :128], h0) + o[:, 128:]
    rf, kf, vf = r_ref[...].astype(F32), k_ref[...].astype(F32), v_ref[...].astype(F32)
    centred = mech - head_sums(mech) * (1.0 / 64)
    spread = head_sums(centred * centred) * (1.0 / 64)
    token = head_sums(rf * kf * own_weight) * vf
    mixed = centred * lax.rsqrt(spread + GROUP_EPS) * hng_ref[...] + token
    mixed = (mixed / (1.0 + jnp.exp(-og_ref[...].astype(F32)))).astype(BF16)

    halves = (pl.ds(0, D // 2), pl.ds(D // 2, D // 2))
    Q = D // 4

    def sum_over_tp(n, a, columns_of, cb, meanwhile):
        other = 1 - core

        def product(q):
            cut = pl.ds(q * Q, Q)
            prod = dot(a, columns_of(q * Q), 1, cb)
            for p in range(8):
                part[p // 2, p % 2, :, cut] = prod[p * ROWS : (p + 1) * ROWS].astype(BF16)
            cp = push(
                part.at[:, other, :, cut], pair_in.at[n, :, :, cut], ps.at[n, q], pr.at[n, q],
                at(dc=1),
            )
            if n == 0:
                pair_sends.append(cp)

        def add_pair(q):
            cut = pl.ds(q * Q, Q)
            landed(pair_in.at[n, :, :, cut], ps.at[n, q], pr.at[n, q])
            mine[n, :, :, cut] = (
                part[:, core, :, cut].astype(F32) + pair_in[n, :, :, cut].astype(F32)
            ).astype(BF16)

        def first_sends(e):
            for d in (2, 1, 3):
                push(
                    mine.at[n, lax.rem(x + d, NX), :, halves[e]], mix_in.at[n, d - 1, :, halves[e]],
                    xs.at[n, e, d - 1], xr.at[n, e, d - 1], at(dx=d),
                )

        product(0)
        product(1)
        add_pair(0)
        product(2)
        add_pair(1)
        first_sends(0)
        product(3)
        meanwhile()
        add_pair(2)
        add_pair(3)
        first_sends(1)
        meanwhile()
        meanwhile()
        total = mine[n, x].astype(F32)
        for d in (1, 3, 2):
            for e in range(2):
                landed(mix_in.at[n, d - 1, :, halves[e]], xs.at[n, e, d - 1], xr.at[n, e, d - 1])
            total = total + mix_in[n, d - 1].astype(F32)
        return total

    def finish_sends():
        for cp in sends:
            cp.wait_send()
        sends.clear()

    service()
    mix = sum_over_tp(0, mixed, lambda c: wo_ref[:, c : c + Q], 0, service)
    mix = mix.astype(BF16).astype(F32)
    fetch.wait()
    after = (resid[...].astype(F32) + mix).astype(BF16).astype(F32)
    factor = lax.rsqrt(jnp.mean(after * after, axis=-1, keepdims=True) + NORM_EPS)
    normed = (after * factor * png_ref[...]).astype(BF16)

    rows_buf[x, core] = normed
    mine_rows = rows_buf.at[x, core]
    for d in (2, 1, 3):
        push(mine_rows, mine_rows, gs.at[d - 1], gr.at[d - 1], at(dx=d))
    push(mine_rows, mine_rows, fs.at[0], fr.at[0], at(dc=1))
    service()
    service()
    for d in (1, 3, 2):
        b = rows_buf.at[lax.rem(x + NX - d, NX), core]
        landed(b, gs.at[d - 1], gr.at[d - 1])
        push(b, b, fs.at[d], fr.at[d], at(dc=1))
    service()
    for d in (0, 1, 3, 2):
        landed(rows_buf.at[lax.rem(x + NX - d, NX), 1 - core], fs.at[d], fr.at[d])
    for j in range(8):
        nrm[j * ROWS : (j + 1) * ROWS] = rows_buf[j // 2, j % 2]

    gate = jnp.zeros((N, FF), F32)
    upper = jnp.zeros((N, FF), F32)
    arrivals = [o for t in range(9) for o in offsets(t)]
    for j in range(8):
        s_last = abs(arrivals[2 * j + 1])
        while turn[0] < min(3 * (s_last + 1) + 3, TURNS):
            one_turn()
        if turn[0] < TURNS:
            one_turn()
        two = arrivals[2 * j : 2 * j + 2]
        for o in two:
            y_end(o)
        cuts = [pl.ds(pl.multiple_of(lax.rem(z + o + NZ, NZ) * 128, 128), 128) for o in two]
        a = jnp.concatenate([nrm[:, cut] for cut in cuts], 1)
        wide = [gu[pl.ds(column(o), NY)] for o in two]
        gate = gate + dot(a, jnp.concatenate([w[:, :W].reshape(128, FF) for w in wide], 0))
        upper = upper + dot(a, jnp.concatenate([w[:, W:].reshape(128, FF) for w in wide], 0))
    assert turn[0] == TURNS
    hidden = (gate / (1.0 + jnp.exp(-gate)) * upper).astype(BF16)
    for cp in pair_sends:
        cp.wait_send()
    sends[:] = [cp for cp in sends if all(cp is not p for p in pair_sends)]
    down = sum_over_tp(1, hidden, lambda c: dn[c // W : (c + Q) // W].reshape(Q, FF), 1, lambda: None)
    out_ref[...] = (after + down).astype(BF16)
    finish_sends()


def per_device(r, k, v, dec, lr, og, stw, hng, wo, res, png, wg, wu, wd):
    vmem = pl.BlockSpec(memory_space=pltpu.VMEM)
    hbm = pl.BlockSpec(memory_space=pl.ANY)
    dma = pltpu.SemaphoreType.DMA
    return pl.pallas_call(
        kernel,
        out_shape=jax.ShapeDtypeStruct((ROWS, D), BF16),
        in_specs=[hbm] * 14,
        out_specs=vmem,
        scratch_shapes=[
            *[pltpu.VMEM((N, 128), BF16)] * 3,
            *[pltpu.VMEM((N, 128), F32)] * 2,
            pltpu.VMEM((N, 128), BF16),
            pltpu.VMEM((2, 64), F32),
            pltpu.VMEM((1, 128), F32),
            pltpu.VMEM((128, D), BF16),
            pltpu.VMEM((1, D), F32),
            pltpu.VMEM((64, 2 * W, FF), BF16),
            pltpu.VMEM((64, W, FF), BF16),
            pltpu.VMEM((2, 4, 64, 256), BF16),
            pltpu.VMEM((4, NY, 16, 256), BF16),
            pltpu.VMEM((NX, NC, ROWS, D), BF16),
            pltpu.VMEM((2, NX, ROWS, D), BF16),
            pltpu.VMEM((2, NX, ROWS, D), BF16),
            pltpu.VMEM((2, 3, ROWS, D), BF16),
            pltpu.VMEM((NX, NC, ROWS, D), BF16),
            pltpu.VMEM((N, D), BF16),
            pltpu.VMEM((N, 256), F32),
            pltpu.VMEM((ROWS, D), BF16),
            dma((4,)), dma((10,)), pltpu.SemaphoreType.REGULAR((2, 3)),
            dma((2, 8)), dma((2, 8)),
            dma((16, 4)), dma((16, 4)),
            dma((3,)), dma((3,)),
            dma((2, 2, 8)), dma((2, 2, 8)),
            dma((4, 3)), dma((4, 3)),
            dma((2, 4)), dma((2, 4)),
            dma((2, 2, 3)), dma((2, 2, 3)),
            dma((3,)), dma((3,)),
            dma((4,)), dma((4,)),
        ],
        compiler_params=pltpu.CompilerParams(
            collective_id=0, has_side_effects=True, vmem_limit_bytes=60 * 1024 * 1024
        ),
        name="layer",
    )(r, k, v, dec, lr, og, stw, hng.reshape(1, 128), wo, res,
      png.reshape(1, D), wg, wu, wd.T)


def solution(mesh):
    torus = Mesh(mesh.devices.reshape(NZ, NY, NX, NC), ("z", "y", "x", "c"))
    sp, tp = ("z", "y"), ("x", "c")
    seq = P(sp, tp)
    return jax.shard_map(
        per_device,
        mesh=torus,
        in_specs=(
            seq, seq, seq, seq, seq, seq, P(tp, None), P(tp), P(tp, None), P(sp, None), P(),
            seq, seq, P(tp, sp),
        ),
        out_specs=P((*sp, *tp), None),
        check_vma=False,
    )
```
